32 devices in a mesh: fs: 8 (over z, y), tp: 4 (over x, core).
Axes of the slice: x: 2, y: 2, z: 4, core: 2. Of those that a mesh axis runs over, the one named last changes fastest.
Arguments:
- saved_inputs: bfloat16 [4096, 3072], P('fs'), may hold values from -6 to 6
- query_cotangent: bfloat16 [4096, 3072], P('fs', 'tp'), may hold values from -0.75 to 0.75
- attn_outputs: bfloat16 [4096, 3072], P('fs', 'tp'), may hold values from -6 to 6
- out_cotangent: bfloat16 [4096, 3072], P('fs'), may hold values from -0.75 to 0.75
- left_factor: bfloat16 [3072, 384], P('fs', 'tp'), may hold values from -0.109375 to 0.109375
- right_factor: bfloat16 [3072, 384], P('fs', 'tp'), may hold values from -0.109375 to 0.109375
- query_master: float32 [3072, 3072], P('fs', 'tp'), may hold values from -0.109375 to 0.109375
- out_master: float32 [3072, 3072], P('tp', 'fs'), may hold values from -0.109375 to 0.109375
- first_moment: float32 [2, 384, 3072], P(None, 'fs', 'tp'), may hold values from -14 to 14
- second_moment: float32 [2, 384, 3072], P(None, 'fs', 'tp'), may hold values from 0.3 to 3
Outputs:
- query_new: float32 [3072, 3072], P('fs', 'tp')
- out_new: float32 [3072, 3072], P('tp', 'fs')
- query_copy: bfloat16 [3072, 3072], P(None, 'tp')
- out_copy: bfloat16 [3072, 3072], P('tp')
- first_new: float32 [2, 384, 3072], P(None, 'fs', 'tp')
- second_new: float32 [2, 384, 3072], P(None, 'fs', 'tp')
The draws below stay inside these ranges and needn't reach their ends.
All inputs are finite; a program needn't handle non-finite values.
Results may differ from the reference program's by a relative error of at most 0.0025.
Values may be sent and summed in bfloat16 or wider, within the bound.
A program may use at most 64 MiB of HBM per device.

```python
import math
import jax
import jax.numpy as jnp
from jax import lax

D = 3072
RANK = 384
QW = 3072
TOKENS = 4096


def draw_first_moment(key, part):
    row_pos = jnp.arange(RANK, dtype=jnp.float32) / RANK
    col_pos = jnp.arange(QW, dtype=jnp.float32) / QW
    base = jnp.clip(jax.random.normal(key, (2, RANK, QW), jnp.float32), -4.0, 4.0)
    growth = 3.0
    spread = growth ** row_pos[:, None] * growth ** col_pos[None, :] / growth
    return (base * spread[None]).astype(jnp.float32)


def shard_levels(own_key, extent, shards, least, high):
    gain = 1.0
    for position, blocks in shards:
        heights = jax.random.uniform(jax.random.fold_in(jax.random.fold_in(own_key, 6), position), (blocks,), jnp.float32, least / len(shards), high / len(shards))
        gain = gain * jnp.repeat(jnp.exp(heights), extent[position] // blocks).reshape((-1,) + (1,) * (len(extent) - 1 - position))
    return gain


def normal_values(own_key, dims, scale, reach, shards=(), held_as=jnp.bfloat16):
    drawn = jax.random.normal(own_key, dims, jnp.float32) * scale
    if len(shards) > 0:
        drawn = shard_levels(own_key, dims, shards, -0.22, 0.18) * drawn
    return jnp.clip(drawn, min=-reach, max=reach).astype(held_as)


def setup_inputs(seed: int = 0) -> dict:
    key_list = jax.random.split(jax.random.key(seed), 11)
    return {
        "saved_inputs": normal_values(key_list[0], (TOKENS, D), 1.0, 6.0, ((0, 8),)),
        "query_cotangent": normal_values(key_list[1], (TOKENS, QW), (8.0 / TOKENS ** 0.5), 0.75, ((0, 8), (1, 4))),
        "attn_outputs": normal_values(key_list[2], (TOKENS, QW), 1.0, 6.0, ((0, 8), (1, 4))),
        "out_cotangent": normal_values(key_list[3], (TOKENS, D), (8.0 / TOKENS ** 0.5), 0.75, ((0, 8),)),
        "left_factor": normal_values(key_list[4], (D, RANK), D ** -0.5, 0.109375, ((0, 8), (1, 4))),
        "right_factor": normal_values(key_list[5], (D, RANK), D ** -0.5, 0.109375, ((0, 8), (1, 4))),
        "query_master": normal_values(key_list[6], (D, QW), D ** -0.5, 0.109375, ((0, 8), (1, 4)), jnp.float32),
        "out_master": normal_values(key_list[7], (QW, D), QW ** -0.5, 0.109375, ((0, 4), (1, 8)), jnp.float32),
        "first_moment": draw_first_moment(jax.random.fold_in(key_list[10], 71), 0),
        "second_moment": jnp.clip(jnp.exp(math.log(3.0) - 2.3025851 * jax.random.uniform(key_list[9], (2, RANK, QW), jnp.float32) ** shard_levels(key_list[9], (2, RANK, QW), ((1, 8), (2, 4)), -0.2, 0.2)), 0.3, 3.0),
    }


def reference(saved_inputs, query_cotangent, attn_outputs, out_cotangent, left_factor, right_factor, query_master, out_master, first_moment, second_moment):
    left_proj = jnp.dot(saved_inputs, left_factor, preferred_element_type=jnp.float32).astype(jnp.bfloat16)
    right_proj = jnp.dot(out_cotangent, right_factor, preferred_element_type=jnp.float32).astype(jnp.bfloat16)
    grad_query = jnp.dot(left_proj.T, query_cotangent, preferred_element_type=jnp.float32)
    grad_output = jnp.dot(right_proj.T, attn_outputs, preferred_element_type=jnp.float32)
    grads = jnp.stack([grad_query, grad_output], axis=0)
    first_new = 0.9 * first_moment + 0.1 * grads
    second_new = 0.99 * second_moment + 0.01 * grads * grads
    direction = first_new / (jnp.sqrt(second_new) + 1e-08)
    scale = lax.rsqrt(lax.optimization_barrier(jnp.mean(direction * direction, axis=(1, 2))) + 1e-06)
    direction_low = direction.astype(jnp.bfloat16)
    step_query = scale[0] * jnp.dot(left_factor, direction_low[0], preferred_element_type=jnp.float32)
    step_output = scale[1] * jnp.dot(direction_low[1].T, right_factor.T, preferred_element_type=jnp.float32)
    query_new = query_master - 0.01 * step_query
    out_new = out_master - 0.01 * step_output
    return (query_new, out_new, query_new.astype(jnp.bfloat16), out_new.astype(jnp.bfloat16), first_new, second_new)
```

```python
import functools

import jax
import jax.numpy as jnp
from jax import lax
from jax.experimental import pallas as pl
from jax.experimental.pallas import tpu as pltpu
from jax.sharding import PartitionSpec as P

MESH = pl.DeviceIdType.MESH
PAIR = 2
NT = (((1,), (1,)), ((), ()))
TN = (((0,), (0,)), ((), ()))


def moment_step(first, second, grads):
    first_next = 0.9 * first + 0.1 * grads
    second_next = 0.99 * second + 0.01 * grads * grads
    return (first_next, second_next, first_next / (jnp.sqrt(second_next) + 1e-08))


def rows(index, size):
    return pl.ds(pl.multiple_of(index * size, size), size)


def peer_along(axis, index):
    if axis == "fs":
        return (index, lax.axis_index("tp"))
    return (lax.axis_index("fs"), index)


class Gather:
    def __init__(self, axis, count, view, sems, own=None):
        self.axis, self.outer, self.view, self.sems = axis, count // PAIR, view, sems
        me = lax.axis_index(axis)
        self.high, self.low = me // PAIR, lax.rem(me, PAIR)
        self.own = view(me) if own is None else own
        self.me = me

    def copy(self, src, dst, stage, slot, target):
        return pltpu.make_async_remote_copy(
            src_ref=src,
            dst_ref=dst,
            send_sem=self.sems.at[stage, 0, slot],
            recv_sem=self.sems.at[stage, 1, slot],
            device_id=peer_along(self.axis, target),
            device_id_type=MESH,
        )

    def index(self, offset, low):
        return lax.rem(self.high + offset, self.outer) * PAIR + low

    def outward(self, offset):
        return self.copy(self.own, self.view(self.me), 0, offset, self.index(offset, self.low))

    def inward(self, offset):
        source = self.index(self.outer - offset, self.low)
        src = self.own if offset == 0 else self.view(source)
        partner = self.high * PAIR + 1 - self.low
        return self.copy(src, self.view(self.me if offset == 0 else source), 1, offset, partner)

    def start_outward(self):
        for offset in range(self.outer - 1, 0, -1):
            self.outward(offset).start()

    def start_inward(self):
        self.inward(0).start()

    def start(self):
        self.start_outward()
        self.start_inward()

    def forward(self):
        for offset in range(self.outer - 1, 0, -1):
            self.outward(offset).wait_recv()
            self.inward(offset).start()

    def finish(self):
        for offset in range(self.outer):
            self.inward(offset).wait_recv()
        for offset in range(1, self.outer):
            self.outward(offset).wait_send()
        for offset in range(self.outer):
            self.inward(offset).wait_send()


def kernel(
    n_fs,
    n_tp,
    saved_hbm,
    outcot_hbm,
    querycot_hbm,
    attn_hbm,
    query_hbm,
    out_hbm,
    factor_ref,
    first_ref,
    second_ref,
    query_out,
    out_out,
    query_copy,
    out_copy,
    first_out,
    second_out,
    factors_ref,
    dirs_ref,
    query_master,
    out_master,
    query_early,
    out_early,
    saved,
    outcot,
    querycot,
    attn,
    proj,
    grad,
    pair_send,
    pair_recv,
    far_send,
    far_recv,
    own_dir,
    square_buf,
    load_sems,
    factor_sems,
    proj_sems,
    columns_sems,
    pair_sems,
    far_sems,
    dir_sems,
    square_sems,
    early_sems,
    late_sems,
):
    me, column = lax.axis_index("fs"), lax.axis_index("tp")
    high, low = me // PAIR, lax.rem(me, PAIR)
    outer = n_fs // PAIR
    part = factor_ref.shape[1]
    width = factor_ref.shape[2]
    depth = first_ref.shape[1]
    loads = [
        pltpu.make_async_copy(src, dst, load_sems.at[i])
        for i, (src, dst) in enumerate(
            (
                (saved_hbm, saved),
                (outcot_hbm, outcot),
                (querycot_hbm, querycot),
                (attn_hbm, attn),
                (query_hbm, query_master),
                (out_hbm, out_master),
            )
        )
    ]
    for load in loads[4:] + loads[:4]:
        load.start()

    peers = [(lax.rem(high + i, outer) * PAIR + low, column) for i in range(1, outer)]
    peers.append((high * PAIR + 1 - low, column))
    peers += [(me, lax.rem(column + i, n_tp)) for i in range(1, n_tp)]
    barrier = pltpu.get_barrier_semaphore()
    for peer in peers:
        pl.semaphore_signal(barrier, inc=1, device_id=peer, device_id_type=MESH)
    pl.semaphore_wait(barrier, len(peers))

    factors = Gather(
        "fs",
        n_fs,
        lambda i: factors_ref.at[:, rows(column, part), rows(i, width)],
        factor_sems,
        own=factor_ref,
    )
    factors.start()
    factors_ref[:, rows(column, part), rows(me, width)] = factor_ref[...]

    half = query_copy.shape[1] // 2
    early = (
        Gather("fs", n_fs, lambda i: query_copy.at[rows(i, width), :half], early_sems.at[0], own=query_early),
        Gather("fs", n_fs, lambda i: out_copy.at[:half, rows(i, width)], early_sems.at[1], own=out_early),
    )
    loads[4].wait()
    query_early[...] = query_master[:, :half].astype(query_early.dtype)
    loads[5].wait()
    out_early[...] = out_master[:half, :].astype(out_early.dtype)
    for gather in early:
        gather.start_outward()
    factors.forward()
    for gather in early:
        gather.start_inward()
    factors.finish()

    gathers = []
    for k, tokens in enumerate((saved, outcot)):
        loads[k].wait()
        part_proj = lax.dot_general(
            factors_ref[k, rows(column, part), :],
            tokens[...],
            NT,
            preferred_element_type=jnp.float32,
        )
        proj[k, rows(column, part), :] = part_proj.astype(proj.dtype)
        gather = Gather(
            "tp", n_tp, lambda i, k=k: proj.at[k, rows(i, part), :], proj_sems.at[k]
        )
        gather.start()
        gathers.append(gather)
    columns = Gather("tp", n_tp, lambda i: factors_ref.at[:, rows(i, part), :], columns_sems)
    for gather in gathers:
        gather.forward()
    columns.start()
    for k, (gather, cot) in enumerate(zip(gathers, (querycot, attn))):
        gather.finish()
        loads[2 + k].wait()
        grad[k, :, :] = jnp.dot(proj[k], cot[...], preferred_element_type=jnp.float32)

    def pair_copy(offset):
        return pltpu.make_async_remote_copy(
            src_ref=pair_send.at[offset],
            dst_ref=pair_recv.at[offset],
            send_sem=pair_sems.at[0, offset],
            recv_sem=pair_sems.at[1, offset],
            device_id=(high * PAIR + 1 - low, column),
            device_id_type=MESH,
        )

    def far_copy(offset):
        return pltpu.make_async_remote_copy(
            src_ref=far_send.at[offset],
            dst_ref=far_recv.at[offset],
            send_sem=far_sems.at[0, offset],
            recv_sem=far_sems.at[1, offset],
            device_id=(lax.rem(high + offset, outer) * PAIR + low, column),
            device_id_type=MESH,
        )

    order = list(range(outer - 1, 0, -1)) + [0]
    for offset in order:
        target = lax.rem(high + offset, outer) * PAIR + 1 - low
        pair_send[offset] = grad[:, rows(target, depth), :].astype(pair_send.dtype)
        pair_copy(offset).start()
    for offset in order:
        target = lax.rem(high + offset, outer) * PAIR + low
        pair_copy(offset).wait_recv()
        both = grad[:, rows(target, depth), :] + pair_recv[offset].astype(jnp.float32)
        if offset:
            far_send[offset] = both.astype(far_send.dtype)
            far_copy(offset).start()
    total = both
    columns.forward()
    for gather in early:
        gather.forward()
    for offset in range(1, outer):
        far_copy(offset).wait_recv()
        total = total + far_recv[offset].astype(jnp.float32)

    first_new, second_new, direction = moment_step(first_ref[...], second_ref[...], total)
    own_dir[...] = direction.astype(own_dir.dtype)
    spread = Gather("fs", n_fs, lambda i: dirs_ref.at[:, rows(i, depth), :], dir_sems, own=own_dir)
    spread.start()
    dirs_ref[:, rows(me, depth), :] = own_dir[...]
    first_out[...] = first_new
    second_out[...] = second_new
    squares = direction * direction
    shape = square_buf.shape[1:]
    row = lax.broadcasted_iota(jnp.int32, shape, 0)
    mine = jnp.where(row == 0, jnp.sum(squares[0]), jnp.sum(squares[1]))

    rounds = (
        [(me, lax.rem(column + i, n_tp)) for i in range(1, n_tp)],
        [(lax.rem(high + i, outer) * PAIR + low, column) for i in range(1, outer)],
        [(high * PAIR + 1 - low, column)],
    )
    slot = 0
    tiny = []
    for stage, targets in enumerate(rounds):
        square_buf[slot] = mine
        base = slot
        copies = []
        for target in targets:
            slot += 1
            copies.append(
                pltpu.make_async_remote_copy(
                    src_ref=square_buf.at[base],
                    dst_ref=square_buf.at[slot],
                    send_sem=square_sems.at[0, slot],
                    recv_sem=square_sems.at[1, slot],
                    device_id=target,
                    device_id_type=MESH,
                )
            )
        for copy in copies:
            copy.start()
        if stage == 1:
            spread.forward()
        for i, copy in enumerate(copies):
            copy.wait_recv()
            mine = mine + square_buf[base + 1 + i]
        tiny += copies
        slot += 1
    spread.finish()
    columns.finish()

    entries = dirs_ref.shape[1] * dirs_ref.shape[2] * n_tp
    scale = 0.01 * lax.rsqrt(mine / entries + 1e-06)
    query_scale, out_scale = scale[0:1, 0:1], scale[1:2, 0:1]

    def step(k, block, part_of_features):
        factor = factors_ref[k, :, rows(block, width)]
        direction = dirs_ref[k, :, part_of_features]
        pair = (factor, direction) if k == 0 else (direction, factor)
        return lax.dot_general(*pair, TN, preferred_element_type=jnp.float32)

    tall, deep = width // 2, half // 2
    late_query = [
        Gather("fs", n_fs, lambda i, p=p: query_copy.at[rows(2 * i + p, tall), half:], late_sems.at[p])
        for p in range(2)
    ]
    late_out = [
        Gather(
            "fs",
            n_fs,
            lambda i, p=p: out_copy.at[half + p * deep : half + (p + 1) * deep, rows(i, width)],
            late_sems.at[2 + p],
        )
        for p in range(2)
    ]
    late = late_query + late_out
    for part_of_features in (slice(half, None), slice(0, half)):
        query_new = query_master[:, part_of_features] - query_scale * step(0, me, part_of_features)
        query_out[:, part_of_features] = query_new
        query_copy[rows(me, width), part_of_features] = query_new.astype(query_copy.dtype)
        if part_of_features.start:
            for gather in late_query:
                gather.start()
        out_new = out_master[part_of_features, :] - out_scale * step(1, me, part_of_features)
        out_out[part_of_features, :] = out_new
        out_copy[part_of_features, rows(me, width)] = out_new.astype(out_copy.dtype)
        if part_of_features.start:
            for gather in late_out:
                gather.start()
    for gather in early:
        gather.finish()

    def finish_block(i, carry):
        block = lax.rem(me + i, n_fs)
        where = rows(block, width)
        query = query_copy[where, :half].astype(jnp.float32)
        query_copy[where, :half] = (query - query_scale * step(0, block, slice(0, half))).astype(query_copy.dtype)
        out = out_copy[:half, where].astype(jnp.float32)
        out_copy[:half, where] = (out - out_scale * step(1, block, slice(0, half))).astype(out_copy.dtype)
        return carry

    lax.fori_loop(1, n_fs, finish_block, 0)
    for gather in late:
        gather.forward()
    for gather in late:
        gather.finish()
    for offset in order:
        pair_copy(offset).wait_send()
        if offset:
            far_copy(offset).wait_send()
    for copy in tiny:
        copy.wait_send()


def store_kernel(*refs):
    count = len(refs) // 2
    sems = refs[-1]
    copies = [pltpu.make_async_copy(refs[i], refs[count + i], sems.at[i]) for i in range(count)]
    for copy in copies:
        copy.start()
    for copy in copies:
        copy.wait()


def fast_body(
    n_fs,
    n_tp,
    saved_inputs,
    query_cotangent,
    attn_outputs,
    out_cotangent,
    left_factor,
    right_factor,
    query_master,
    out_master,
    first_moment,
    second_moment,
):
    tokens, model = saved_inputs.shape
    features = query_cotangent.shape[1]
    width, part = left_factor.shape
    depth = first_moment.shape[1]
    rank = part * n_tp
    outer = n_fs // PAIR
    half = features // 2
    low, wide = jnp.bfloat16, jnp.float32
    vmem = pl.BlockSpec(memory_space=pltpu.VMEM)
    anywhere = pl.BlockSpec(memory_space=pl.ANY)
    dma = pltpu.SemaphoreType.DMA
    tiny_slots = n_tp + outer + PAIR
    factor = jnp.stack([left_factor.T, right_factor.T])
    results = pl.pallas_call(
        functools.partial(kernel, n_fs, n_tp),
        out_shape=(
            pltpu.VMEM((width, features), wide),
            pltpu.VMEM((features, width), wide),
            pltpu.VMEM((model, features), low),
            pltpu.VMEM((features, model), low),
            pltpu.VMEM(first_moment.shape, wide),
            pltpu.VMEM(first_moment.shape, wide),
        ),
        in_specs=[anywhere] * 6 + [vmem] * 3,
        out_specs=(vmem,) * 6,
        scratch_shapes=[
            pltpu.VMEM((2, rank, model), low),
            pltpu.VMEM((2, rank, features), low),
            pltpu.VMEM((width, features), wide),
            pltpu.VMEM((features, width), wide),
            pltpu.VMEM((width, half), low),
            pltpu.VMEM((half, width), low),
            pltpu.VMEM((tokens, model), low),
            pltpu.VMEM((tokens, model), low),
            pltpu.VMEM((tokens, features), low),
            pltpu.VMEM((tokens, features), low),
            pltpu.VMEM((2, rank, tokens), low),
            pltpu.VMEM((2, rank, features), wide),
            pltpu.VMEM((outer, 2, depth, features), low),
            pltpu.VMEM((outer, 2, depth, features), low),
            pltpu.VMEM((outer, 2, depth, features), low),
            pltpu.VMEM((outer, 2, depth, features), low),
            pltpu.VMEM((2, depth, features), low),
            pltpu.VMEM((tiny_slots, 8, 128), wide),
            dma((6,)),
            dma((2, 2, outer)),
            dma((2, 2, 2, n_tp // PAIR)),
            dma((2, 2, n_tp // PAIR)),
            dma((2, outer)),
            dma((2, outer)),
            dma((2, 2, outer)),
            dma((2, tiny_slots)),
            dma((2, 2, 2, outer)),
            dma((4, 2, 2, outer)),
        ],
        compiler_params=pltpu.CompilerParams(
            collective_id=0, has_side_effects=True, vmem_limit_bytes=46 * 2**20
        ),
        cost_estimate=pl.CostEstimate(
            flops=4 * tokens * rank * (model + features), bytes_accessed=200 * 2**20, transcendentals=0
        ),
    )(
        saved_inputs,
        out_cotangent,
        query_cotangent,
        attn_outputs,
        query_master,
        out_master,
        factor,
        first_moment,
        second_moment,
    )
    return pl.pallas_call(
        store_kernel,
        out_shape=tuple(jax.ShapeDtypeStruct(r.shape, r.dtype) for r in results),
        in_specs=[vmem] * len(results),
        out_specs=(anywhere,) * len(results),
        scratch_shapes=[dma((len(results),))],
        compiler_params=pltpu.CompilerParams(vmem_limit_bytes=2**20),
        cost_estimate=pl.CostEstimate(flops=2**20, bytes_accessed=13 * 2**20, transcendentals=0),
    )(*(pltpu.with_memory_space_constraint(r, pltpu.VMEM) for r in results))


def plain_body(
    saved_inputs,
    query_cotangent,
    attn_outputs,
    out_cotangent,
    left_factor,
    right_factor,
    query_master,
    out_master,
    first_moment,
    second_moment,
):
    left_part = jnp.dot(
        saved_inputs,
        lax.all_gather(left_factor, "fs", axis=0, tiled=True),
        preferred_element_type=jnp.float32,
    )
    right_part = jnp.dot(
        out_cotangent,
        lax.all_gather(right_factor, "fs", axis=0, tiled=True),
        preferred_element_type=jnp.float32,
    )
    left_proj, right_proj, left_rows, right_rows = (
        lax.all_gather(left_part.astype(jnp.bfloat16), "tp", axis=1, tiled=True),
        lax.all_gather(right_part.astype(jnp.bfloat16), "tp", axis=1, tiled=True),
        lax.all_gather(left_factor, "tp", axis=1, tiled=True),
        lax.all_gather(right_factor, "tp", axis=1, tiled=True),
    )
    depth = first_moment.shape[1]
    grad_query = lax.dot_general(left_proj, query_cotangent, TN, preferred_element_type=jnp.float32)
    grad_output = lax.dot_general(right_proj, attn_outputs, TN, preferred_element_type=jnp.float32)
    summed = lax.psum_scatter(
        jnp.stack([grad_query, grad_output], axis=1), "fs", scatter_dimension=0, tiled=True
    )
    grads = jnp.transpose(summed, (1, 0, 2))
    first_new, second_new, own_direction = moment_step(first_moment, second_moment, grads)
    direction_all = lax.all_gather(own_direction.astype(jnp.bfloat16), "fs", axis=1, tiled=True)
    squares = jnp.sum(own_direction * own_direction, axis=(1, 2))
    total = lax.psum(squares, ("fs", "tp"))
    entries = depth * lax.axis_size("fs") * own_direction.shape[2] * lax.axis_size("tp")
    scale = lax.rsqrt(total / entries + 1e-06)
    step_query = scale[0] * jnp.dot(left_rows, direction_all[0], preferred_element_type=jnp.float32)
    step_output = scale[1] * lax.dot_general(
        direction_all[1], right_rows, (((0,), (1,)), ((), ())), preferred_element_type=jnp.float32
    )
    query_new = query_master - 0.01 * step_query
    out_new = out_master - 0.01 * step_output
    query_copy, out_copy = (
        lax.all_gather(query_new.astype(jnp.bfloat16), "fs", axis=0, tiled=True),
        lax.all_gather(out_new.astype(jnp.bfloat16), "fs", axis=1, tiled=True),
    )
    return (query_new, out_new, query_copy, out_copy, first_new, second_new)


def choose_body(n_fs, n_tp, *args):
    left_factor, first_moment = args[4], args[8]
    model, part = args[0].shape[1], left_factor.shape[1]
    aligned = part % 16 == 0 and first_moment.shape[1] % 16 == 0
    aligned = aligned and model // n_fs % 128 == 0 and first_moment.shape[2] % 256 == 0
    aligned = aligned and model // n_fs % 32 == 0 and first_moment.shape[2] % 64 == 0
    if aligned and n_fs % PAIR == 0 and n_tp % PAIR == 0:
        return fast_body(n_fs, n_tp, *args)
    return plain_body(*args)


def solution(mesh):
    return jax.shard_map(
        functools.partial(choose_body, mesh.shape["fs"], mesh.shape["tp"]),
        mesh=mesh,
        in_specs=(
            P("fs", None),
            P("fs", "tp"),
            P("fs", "tp"),
            P("fs", None),
            P("fs", "tp"),
            P("fs", "tp"),
            P("fs", "tp"),
            P("tp", "fs"),
            P(None, "fs", "tp"),
            P(None, "fs", "tp"),
        ),
        out_specs=(
            P("fs", "tp"),
            P("tp", "fs"),
            P(None, "tp"),
            P("tp", None),
            P(None, "fs", "tp"),
            P(None, "fs", "tp"),
        ),
        check_vma=False,
    )
```

```python
import functools

import jax
import jax.numpy as jnp
from jax import lax
from jax.experimental import pallas as pl
from jax.experimental.pallas import tpu as pltpu
from jax.sharding import PartitionSpec as P

MESH = pl.DeviceIdType.MESH
PAIR = 2
LINE = 4
LANES = 128
EARLY_QUERY = 1
EARLY_OUT = 1
NT = (((1,), (1,)), ((), ()))
TN = (((0,), (0,)), ((), ()))


def moment_step(first, second, grads):
    first_next = 0.9 * first + 0.1 * grads
    second_next = 0.99 * second + 0.01 * grads * grads
    return (first_next, second_next, first_next / (jnp.sqrt(second_next) + 1e-08))


def rows(index, size):
    return pl.ds(pl.multiple_of(index * size, size), size)


def peer_along(axis, index):
    if axis == "fs":
        return (index, lax.axis_index("tp"))
    return (lax.axis_index("fs"), index)


class Gather:
    def __init__(self, axis, count, view, sems, own=None):
        self.axis, self.outer, self.view, self.sems = axis, count // PAIR, view, sems
        me = lax.axis_index(axis)
        self.high, self.low = me // PAIR, lax.rem(me, PAIR)
        self.own = view(me) if own is None else own
        self.me = me

    def copy(self, src, dst, stage, slot, target):
        return pltpu.make_async_remote_copy(
            src_ref=src,
            dst_ref=dst,
            send_sem=self.sems.at[stage, 0, slot],
            recv_sem=self.sems.at[stage, 1, slot],
            device_id=peer_along(self.axis, target),
            device_id_type=MESH,
        )

    def index(self, offset, low):
        return lax.rem(self.high + offset, self.outer) * PAIR + low

    def outward(self, offset):
        return self.copy(self.own, self.view(self.me), 0, offset, self.index(offset, self.low))

    def inward(self, offset):
        source = self.index(self.outer - offset, self.low)
        src = self.own if offset == 0 else self.view(source)
        partner = self.high * PAIR + 1 - self.low
        return self.copy(src, self.view(self.me if offset == 0 else source), 1, offset, partner)

    def start_outward(self):
        for offset in range(self.outer - 1, 0, -1):
            self.outward(offset).start()

    def start_inward(self):
        self.inward(0).start()

    def start(self):
        self.start_outward()
        self.start_inward()

    def forward(self):
        for offset in range(self.outer - 1, 0, -1):
            self.outward(offset).wait_recv()
            self.inward(offset).start()

    def finish(self):
        for offset in range(self.outer):
            self.inward(offset).wait_recv()
        for offset in range(1, self.outer):
            self.outward(offset).wait_send()
        for offset in range(self.outer):
            self.inward(offset).wait_send()


class Place:
    def __init__(self, outer):
        me, self.column = lax.axis_index("fs"), lax.axis_index("tp")
        self.me, self.low, self.outer = me, lax.rem(me, PAIR), outer
        self.z = me // PAIR
        self.near = self.z + 1 - 2 * lax.rem(self.z, 2)
        self.cross = outer - 1 - self.z
        self.skew = outer - 1 - self.near
        self.end = jnp.logical_or(self.z == 0, self.z == outer - 1)
        self.inner = jnp.logical_not(self.end)

    def same(self, z):
        return z * PAIR + self.low

    def other(self, z):
        return z * PAIR + 1 - self.low


class Spread:
    def __init__(self, place, view, sends, recvs, odd, own=None):
        self.place, self.view, self.sends, self.recvs, self.odd = place, view, sends, recvs, odd
        self.own = view(place.me) if own is None else own

    def copy(self, block, send, recv, target):
        return pltpu.make_async_remote_copy(
            src_ref=self.own if block is None else self.view(block),
            dst_ref=self.view(self.place.me if block is None else block),
            send_sem=self.sends.at[send],
            recv_sem=self.recvs.at[recv],
            device_id=(target, self.place.column),
            device_id_type=MESH,
        )

    def to_skew(self):
        return self.copy(None, 0, 0, self.place.same(self.place.skew))

    def to_near(self):
        return self.copy(None, 1, 1, self.place.same(self.place.near))

    def to_cross(self):
        return self.copy(None, 2, 2, self.place.same(self.place.cross))

    def to_pair(self):
        return self.copy(None, 3, 3, self.place.other(self.place.z))

    def pair_skew(self):
        return self.copy(self.place.same(self.place.skew), 4, 4, self.place.other(self.place.z))

    def pair_near(self):
        return self.copy(self.place.same(self.place.near), 5, 5, self.place.other(self.place.z))

    def pair_cross(self):
        return self.copy(self.place.same(self.place.cross), 6, 6, self.place.other(self.place.z))

    def relay_skew(self):
        return self.copy(self.place.same(self.place.skew), 7, 2, self.place.same(self.place.near))

    def relay_pair(self):
        return self.copy(self.place.other(self.place.z), 8, 5, self.place.same(self.place.near))

    def when(self, condition, action):
        if condition is True:
            action()
        elif condition is not False:
            pl.when(condition)(action)

    def launch(self):
        self.to_pair().start()
        self.to_skew().start()
        self.to_near().start()
        self.when(self.place.inner, lambda: self.to_cross().start())

    def relay(self):
        self.to_skew().wait_recv()
        self.when(self.place.inner, lambda: self.relay_skew().start())
        self.pair_skew().start()
        self.to_near().wait_recv()
        self.when(False if self.odd else self.place.end, lambda: self.pair_near().start())
        self.to_pair().wait_recv()
        self.when(True if self.odd else self.place.end, lambda: self.relay_pair().start())

    def relay_last(self):
        self.to_cross().wait_recv()
        self.pair_cross().start()

    def collect(self):
        self.pair_skew().wait_recv()
        self.pair_near().wait_recv()
        self.pair_cross().wait_recv()

    def drain(self):
        self.to_pair().wait_send()
        self.to_skew().wait_send()
        self.to_near().wait_send()
        self.pair_skew().wait_send()
        self.pair_cross().wait_send()
        self.when(self.place.inner, lambda: self.to_cross().wait_send())
        self.when(self.place.inner, lambda: self.relay_skew().wait_send())
        self.when(False if self.odd else self.place.end, lambda: self.pair_near().wait_send())
        self.when(True if self.odd else self.place.end, lambda: self.relay_pair().wait_send())


def kernel(
    n_fs,
    n_tp,
    early_query,
    early_out,
    saved_hbm,
    outcot_hbm,
    querycot_hbm,
    attn_hbm,
    query_hbm,
    out_hbm,
    factor_ref,
    first_ref,
    second_ref,
    query_out,
    out_out,
    query_copy,
    out_copy,
    first_out,
    second_out,
    factors_ref,
    own_rows,
    dirs_ref,
    query_master,
    out_master,
    query_early,
    out_early,
    saved,
    outcot,
    querycot,
    attn,
    proj,
    grad,
    pair_send,
    pair_recv,
    far_send,
    far_recv,
    own_dir,
    square_buf,
    load_sems,
    rows_sems,
    proj_sems,
    columns_sems,
    pair_sems,
    far_sems,
    square_sems,
    spread_sends,
    spread_recvs,
):
    outer = n_fs // PAIR
    place = Place(outer)
    me, column, high, low = place.me, place.column, place.z, place.low
    part = factor_ref.shape[1]
    width = factor_ref.shape[2]
    depth = first_ref.shape[1]
    features = grad.shape[2]
    pieces = width // LANES
    tall, deep = LANES, features // pieces
    loads = [
        pltpu.make_async_copy(src, dst, load_sems.at[i])
        for i, (src, dst) in enumerate(
            (
                (saved_hbm, saved),
                (outcot_hbm, outcot),
                (querycot_hbm, querycot),
                (attn_hbm, attn),
                (query_hbm, query_master),
                (out_hbm, out_master),
            )
        )
    ]
    for load in loads:
        load.start()

    fs_peers = [(lax.rem(me + i, n_fs), column) for i in range(1, n_fs)]
    tp_peers = [(me, lax.rem(column + i, n_tp)) for i in range(1, n_tp)]
    barrier = pltpu.get_barrier_semaphore()
    for peer in fs_peers + tp_peers:
        pl.semaphore_signal(barrier, inc=1, device_id=peer, device_id_type=MESH)
    pl.semaphore_wait(barrier, len(fs_peers) + len(tp_peers))

    def spread(slot, view, odd, own=None):
        return Spread(place, view, spread_sends.at[slot], spread_recvs.at[slot], odd, own)

    factors = [
        spread(
            k,
            lambda i, k=k: factors_ref.at[k, rows(column, part), rows(i, width)],
            k == 1,
            factor_ref.at[k],
        )
        for k in range(2)
    ]
    for gather in factors:
        gather.launch()
    own_columns = Gather("tp", n_tp, lambda i: own_rows.at[:, rows(i, part), :], rows_sems, own=factor_ref)
    own_columns.start()
    factors_ref[:, rows(column, part), rows(me, width)] = factor_ref[...]
    own_rows[:, rows(column, part), :] = factor_ref[...]

    def query_piece(i, own=None):
        return spread(
            4 + i,
            lambda j: query_copy.at[pl.ds(pl.multiple_of(j * width + i * tall, tall), tall), :],
            i % 2 == 1,
            own,
        )

    def out_piece(i, own=None):
        return spread(
            4 + pieces + i,
            lambda j: out_copy.at[i * deep : (i + 1) * deep, rows(j, width)],
            (pieces + i) % 2 == 1,
            own,
        )

    early_q = [query_piece(i, query_early.at[i]) for i in range(early_query)]
    early_o = [out_piece(i, out_early.at[i]) for i in range(early_out)]
    late_q = [query_piece(i) for i in range(early_query, pieces)]
    late_o = [out_piece(i) for i in range(early_out, pieces)]

    for gather in factors:
        gather.relay()
    loads[4].wait()
    for i in range(early_query):
        query_early[i] = query_master[i * tall : (i + 1) * tall, :].astype(query_early.dtype)
    loads[5].wait()
    for i in range(early_out):
        out_early[i] = out_master[i * deep : (i + 1) * deep, :].astype(out_early.dtype)
    for gather in factors:
        gather.relay_last()
    for gather in early_q:
        gather.launch()
    own_columns.forward()

    gathers = []
    for k, tokens in enumerate((saved, outcot)):
        factors[k].collect()
        loads[k].wait()
        part_proj = lax.dot_general(
            factors_ref[k, rows(column, part), :],
            tokens[...],
            NT,
            preferred_element_type=jnp.float32,
        )
        proj[k, rows(column, part), :] = part_proj.astype(proj.dtype)
        gather = Gather(
            "tp", n_tp, lambda i, k=k: proj.at[k, rows(i, part), :], proj_sems.at[k]
        )
        gather.start()
        gathers.append(gather)

    def pair_copy(offset, k):
        return pltpu.make_async_remote_copy(
            src_ref=pair_send.at[offset, k],
            dst_ref=pair_recv.at[offset, k],
            send_sem=pair_sems.at[0, offset, k],
            recv_sem=pair_sems.at[1, offset, k],
            device_id=(high * PAIR + 1 - low, column),
            device_id_type=MESH,
        )

    def far_copy(offset, k):
        return pltpu.make_async_remote_copy(
            src_ref=far_send.at[offset, k],
            dst_ref=far_recv.at[offset, k],
            send_sem=far_sems.at[0, offset, k],
            recv_sem=far_sems.at[1, offset, k],
            device_id=(lax.rem(high + offset, outer) * PAIR + low, column),
            device_id_type=MESH,
        )

    columns = Gather("tp", n_tp, lambda i: factors_ref.at[:, rows(i, part), :], columns_sems)
    order = list(range(outer - 1, 0, -1)) + [0]
    for k, (gather, cot) in enumerate(zip(gathers, (querycot, attn))):
        gather.forward()
        if k == 1:
            columns.start()
        gather.finish()
        loads[2 + k].wait()
        grad[k, :, :] = jnp.dot(proj[k], cot[...], preferred_element_type=jnp.float32)
        for offset in order:
            target = lax.rem(high + offset, outer) * PAIR + 1 - low
            pair_send[offset, k] = grad[k, rows(target, depth), :].astype(pair_send.dtype)
            pair_copy(offset, k).start()
    totals = []
    for k in range(2):
        for offset in order:
            target = lax.rem(high + offset, outer) * PAIR + low
            pair_copy(offset, k).wait_recv()
            both = grad[k, rows(target, depth), :] + pair_recv[offset, k].astype(jnp.float32)
            if offset:
                far_send[offset, k] = both.astype(far_send.dtype)
                far_copy(offset, k).start()
        totals.append(both)
    for gather in early_q:
        gather.relay()
    for k in range(2):
        for offset in range(1, outer):
            far_copy(offset, k).wait_recv()
            totals[k] = totals[k] + far_recv[offset, k].astype(jnp.float32)

    shape = square_buf.shape[1:]
    row = lax.broadcasted_iota(jnp.int32, shape, 0)
    mine = jnp.zeros(shape, jnp.float32)
    for k in range(2):
        first_new, second_new, direction = moment_step(first_ref[k], second_ref[k], totals[k])
        own_dir[k] = direction.astype(own_dir.dtype)
        first_out[k] = first_new
        second_out[k] = second_new
        mine = jnp.where(row == k, jnp.sum(direction * direction), mine)

    def square_copies(base, targets):
        return [
            pltpu.make_async_remote_copy(
                src_ref=square_buf.at[base],
                dst_ref=square_buf.at[base + 1 + i],
                send_sem=square_sems.at[0, base + 1 + i],
                recv_sem=square_sems.at[1, base + 1 + i],
                device_id=target,
                device_id_type=MESH,
            )
            for i, target in enumerate(targets)
        ]

    square_buf[0] = mine
    square_fs = square_copies(0, fs_peers)
    for copy in square_fs:
        copy.start()
    dirs = [
        spread(2 + k, lambda i, k=k: dirs_ref.at[k, rows(i, depth), :], k == 1, own_dir.at[k]) for k in range(2)
    ]
    for gather in dirs:
        gather.launch()
    dirs_ref[:, rows(me, depth), :] = own_dir[...]
    for i, copy in enumerate(square_fs):
        copy.wait_recv()
        mine = mine + square_buf[1 + i]
    square_buf[n_fs] = mine
    square_tp = square_copies(n_fs, tp_peers)
    for copy in square_tp:
        copy.start()
    for gather in dirs:
        gather.relay()
    for gather in early_q:
        gather.relay_last()
    for gather in dirs:
        gather.relay_last()
    for gather in early_o:
        gather.launch()
    for i, copy in enumerate(square_tp):
        copy.wait_recv()
        mine = mine + square_buf[n_fs + 1 + i]
    entries = dirs_ref.shape[1] * dirs_ref.shape[2] * n_tp
    scale = 0.01 * lax.rsqrt(mine / entries + 1e-06)
    scales = (scale[0:1, 0:1], scale[1:2, 0:1])
    own_columns.finish()
    for gather in dirs:
        gather.collect()

    query_new = query_master[...] - scales[0] * lax.dot_general(
        own_rows[0], dirs_ref[0], TN, preferred_element_type=jnp.float32
    )
    query_out[...] = query_new
    query_copy[rows(me, width), :] = query_new.astype(query_copy.dtype)
    for gather in late_q:
        gather.launch()
    out_new = out_master[...] - scales[1] * lax.dot_general(
        dirs_ref[1], own_rows[1], TN, preferred_element_type=jnp.float32
    )
    out_out[...] = out_new
    out_copy[:, rows(me, width)] = out_new.astype(out_copy.dtype)
    for gather in late_o:
        gather.launch()

    columns.forward()
    for gather in early_o + late_q + late_o:
        gather.relay()
    for gather in early_o + late_q + late_o:
        gather.relay_last()
    columns.finish()

    for gather in early_q + early_o:
        gather.collect()
        gather.drain()

    def finish_block(i, carry):
        block = lax.rem(me + i, n_fs)
        for j in range(early_query):
            where = pl.ds(pl.multiple_of(block * width + j * tall, tall), tall)
            step = lax.dot_general(
                factors_ref[0, :, where], dirs_ref[0], TN, preferred_element_type=jnp.float32
            )
            query = query_copy[where, :].astype(jnp.float32)
            query_copy[where, :] = (query - scales[0] * step).astype(query_copy.dtype)
        for j in range(early_out):
            band = slice(j * deep, (j + 1) * deep)
            step = lax.dot_general(
                dirs_ref[1, :, band],
                factors_ref[1, :, rows(block, width)],
                TN,
                preferred_element_type=jnp.float32,
            )
            out = out_copy[band, rows(block, width)].astype(jnp.float32)
            out_copy[band, rows(block, width)] = (out - scales[1] * step).astype(out_copy.dtype)
        return carry

    lax.fori_loop(1, n_fs, finish_block, 0)
    for gather in late_q + late_o:
        gather.collect()
    for gather in factors + dirs + late_q + late_o:
        gather.drain()
    for k in range(2):
        for offset in order:
            pair_copy(offset, k).wait_send()
            if offset:
                far_copy(offset, k).wait_send()
    for copy in square_fs + square_tp:
        copy.wait_send()


def store_kernel(*refs):
    count = len(refs) // 2
    sems = refs[-1]
    copies = [pltpu.make_async_copy(refs[i], refs[count + i], sems.at[i]) for i in range(count)]
    for copy in copies:
        copy.start()
    for copy in copies:
        copy.wait()


def fast_body(
    n_fs,
    n_tp,
    saved_inputs,
    query_cotangent,
    attn_outputs,
    out_cotangent,
    left_factor,
    right_factor,
    query_master,
    out_master,
    first_moment,
    second_moment,
):
    tokens, model = saved_inputs.shape
    features = query_cotangent.shape[1]
    width, part = left_factor.shape
    depth = first_moment.shape[1]
    rank = part * n_tp
    outer = n_fs // PAIR
    pieces = width // LANES
    low, wide = jnp.bfloat16, jnp.float32
    vmem = pl.BlockSpec(memory_space=pltpu.VMEM)
    anywhere = pl.BlockSpec(memory_space=pl.ANY)
    dma = pltpu.SemaphoreType.DMA
    factor = jnp.stack([left_factor.T, right_factor.T])
    results = pl.pallas_call(
        functools.partial(kernel, n_fs, n_tp, EARLY_QUERY, EARLY_OUT),
        out_shape=(
            pltpu.VMEM((width, features), wide),
            pltpu.VMEM((features, width), wide),
            pltpu.VMEM((model, features), low),
            pltpu.VMEM((features, model), low),
            pltpu.VMEM(first_moment.shape, wide),
            pltpu.VMEM(first_moment.shape, wide),
        ),
        in_specs=[anywhere] * 6 + [vmem] * 3,
        out_specs=(vmem,) * 6,
        scratch_shapes=[
            pltpu.VMEM((2, rank, model), low),
            pltpu.VMEM((2, rank, width), low),
            pltpu.VMEM((2, rank, features), low),
            pltpu.VMEM((width, features), wide),
            pltpu.VMEM((features, width), wide),
            pltpu.VMEM((max(EARLY_QUERY, 1), LANES, features), low),
            pltpu.VMEM((max(EARLY_OUT, 1), features // pieces, width), low),
            pltpu.VMEM((tokens, model), low),
            pltpu.VMEM((tokens, model), low),
            pltpu.VMEM((tokens, features), low),
            pltpu.VMEM((tokens, features), low),
            pltpu.VMEM((2, rank, tokens), low),
            pltpu.VMEM((2, rank, features), wide),
            pltpu.VMEM((outer, 2, depth, features), low),
            pltpu.VMEM((outer, 2, depth, features), low),
            pltpu.VMEM((outer, 2, depth, features), low),
            pltpu.VMEM((outer, 2, depth, features), low),
            pltpu.VMEM((2, depth, features), low),
            pltpu.VMEM((n_fs + n_tp, 8, 128), wide),
            dma((6,)),
            dma((2, 2, n_tp // PAIR)),
            dma((2, 2, 2, n_tp // PAIR)),
            dma((2, 2, n_tp // PAIR)),
            dma((2, outer, 2)),
            dma((2, outer, 2)),
            dma((2, n_fs + n_tp)),
            dma((4 + 2 * pieces, 9)),
            dma((4 + 2 * pieces, 7)),
        ],
        compiler_params=pltpu.CompilerParams(
            collective_id=0, has_side_effects=True, vmem_limit_bytes=46 * 2**20
        ),
        cost_estimate=pl.CostEstimate(
            flops=4 * tokens * rank * (model + features), bytes_accessed=200 * 2**20, transcendentals=0
        ),
    )(
        saved_inputs,
        out_cotangent,
        query_cotangent,
        attn_outputs,
        query_master,
        out_master,
        factor,
        first_moment,
        second_moment,
    )
    return pl.pallas_call(
        store_kernel,
        out_shape=tuple(jax.ShapeDtypeStruct(r.shape, r.dtype) for r in results),
        in_specs=[vmem] * len(results),
        out_specs=(anywhere,) * len(results),
        scratch_shapes=[dma((len(results),))],
        compiler_params=pltpu.CompilerParams(vmem_limit_bytes=2**20),
        cost_estimate=pl.CostEstimate(flops=2**20, bytes_accessed=13 * 2**20, transcendentals=0),
    )(*(pltpu.with_memory_space_constraint(r, pltpu.VMEM) for r in results))


def plain_body(
    saved_inputs,
    query_cotangent,
    attn_outputs,
    out_cotangent,
    left_factor,
    right_factor,
    query_master,
    out_master,
    first_moment,
    second_moment,
):
    left_part = jnp.dot(
        saved_inputs,
        lax.all_gather(left_factor, "fs", axis=0, tiled=True),
        preferred_element_type=jnp.float32,
    )
    right_part = jnp.dot(
        out_cotangent,
        lax.all_gather(right_factor, "fs", axis=0, tiled=True),
        preferred_element_type=jnp.float32,
    )
    left_proj, right_proj, left_rows, right_rows = (
        lax.all_gather(left_part.astype(jnp.bfloat16), "tp", axis=1, tiled=True),
        lax.all_gather(right_part.astype(jnp.bfloat16), "tp", axis=1, tiled=True),
        lax.all_gather(left_factor, "tp", axis=1, tiled=True),
        lax.all_gather(right_factor, "tp", axis=1, tiled=True),
    )
    depth = first_moment.shape[1]
    grad_query = lax.dot_general(left_proj, query_cotangent, TN, preferred_element_type=jnp.float32)
    grad_output = lax.dot_general(right_proj, attn_outputs, TN, preferred_element_type=jnp.float32)
    summed = lax.psum_scatter(
        jnp.stack([grad_query, grad_output], axis=1), "fs", scatter_dimension=0, tiled=True
    )
    grads = jnp.transpose(summed, (1, 0, 2))
    first_new, second_new, own_direction = moment_step(first_moment, second_moment, grads)
    direction_all = lax.all_gather(own_direction.astype(jnp.bfloat16), "fs", axis=1, tiled=True)
    squares = jnp.sum(own_direction * own_direction, axis=(1, 2))
    total = lax.psum(squares, ("fs", "tp"))
    entries = depth * lax.axis_size("fs") * own_direction.shape[2] * lax.axis_size("tp")
    scale = lax.rsqrt(total / entries + 1e-06)
    step_query = scale[0] * jnp.dot(left_rows, direction_all[0], preferred_element_type=jnp.float32)
    step_output = scale[1] * lax.dot_general(
        direction_all[1], right_rows, (((0,), (1,)), ((), ())), preferred_element_type=jnp.float32
    )
    query_new = query_master - 0.01 * step_query
    out_new = out_master - 0.01 * step_output
    query_copy, out_copy = (
        lax.all_gather(query_new.astype(jnp.bfloat16), "fs", axis=0, tiled=True),
        lax.all_gather(out_new.astype(jnp.bfloat16), "fs", axis=1, tiled=True),
    )
    return (query_new, out_new, query_copy, out_copy, first_new, second_new)


def choose_body(n_fs, n_tp, *args):
    left_factor, first_moment = args[4], args[8]
    model, part = args[0].shape[1], left_factor.shape[1]
    aligned = part % 16 == 0 and first_moment.shape[1] % 16 == 0
    aligned = aligned and model // n_fs % 128 == 0 and first_moment.shape[2] % 256 == 0
    aligned = aligned and first_moment.shape[2] % (model // n_fs) == 0
    if aligned and n_fs == PAIR * LINE and n_tp % PAIR == 0:
        return fast_body(n_fs, n_tp, *args)
    return plain_body(*args)


def solution(mesh):
    return jax.shard_map(
        functools.partial(choose_body, mesh.shape["fs"], mesh.shape["tp"]),
        mesh=mesh,
        in_specs=(
            P("fs", None),
            P("fs", "tp"),
            P("fs", "tp"),
            P("fs", None),
            P("fs", "tp"),
            P("fs", "tp"),
            P("fs", "tp"),
            P("tp", "fs"),
            P(None, "fs", "tp"),
            P(None, "fs", "tp"),
        ),
        out_specs=(
            P("fs", "tp"),
            P("tp", "fs"),
            P(None, "tp"),
            P("tp", None),
            P(None, "fs", "tp"),
            P(None, "fs", "tp"),
        ),
        check_vma=False,
    )
```

```python
import functools

import jax
import jax.numpy as jnp
from jax import lax
from jax.experimental import pallas as pl
from jax.experimental.pallas import tpu as pltpu
from jax.sharding import PartitionSpec as P

MESH = pl.DeviceIdType.MESH
PAIR = 2
LINE = 4
LANES = 128
EARLY_QUERY = 1
EARLY_OUT = 1
STORES = 4
QUERY_ODD = (True,False,True)
OUT_ODD = (True,False,True)
NT = (((1,), (1,)), ((), ()))
TN = (((0,), (0,)), ((), ()))


def moment_step(first, second, grads):
    first_next = 0.9 * first + 0.1 * grads
    second_next = 0.99 * second + 0.01 * grads * grads
    return (first_next, second_next, first_next / (jnp.sqrt(second_next) + 1e-08))


def rows(index, size):
    return pl.ds(pl.multiple_of(index * size, size), size)


def peer_along(axis, index):
    if axis == "fs":
        return (index, lax.axis_index("tp"))
    return (lax.axis_index("fs"), index)


class Gather:
    def __init__(self, axis, count, view, sems, own=None):
        self.axis, self.outer, self.view, self.sems = axis, count // PAIR, view, sems
        me = lax.axis_index(axis)
        self.high, self.low = me // PAIR, lax.rem(me, PAIR)
        self.own = view(me) if own is None else own
        self.me = me

    def copy(self, src, dst, stage, slot, target):
        return pltpu.make_async_remote_copy(
            src_ref=src,
            dst_ref=dst,
            send_sem=self.sems.at[stage, 0, slot],
            recv_sem=self.sems.at[stage, 1, slot],
            device_id=peer_along(self.axis, target),
            device_id_type=MESH,
        )

    def index(self, offset, low):
        return lax.rem(self.high + offset, self.outer) * PAIR + low

    def outward(self, offset):
        return self.copy(self.own, self.view(self.me), 0, offset, self.index(offset, self.low))

    def inward(self, offset):
        source = self.index(self.outer - offset, self.low)
        src = self.own if offset == 0 else self.view(source)
        partner = self.high * PAIR + 1 - self.low
        return self.copy(src, self.view(self.me if offset == 0 else source), 1, offset, partner)

    def start_outward(self):
        for offset in range(self.outer - 1, 0, -1):
            self.outward(offset).start()

    def start_inward(self):
        self.inward(0).start()

    def start(self):
        self.start_outward()
        self.start_inward()

    def forward(self):
        for offset in range(self.outer - 1, 0, -1):
            self.outward(offset).wait_recv()
            self.inward(offset).start()

    def finish(self):
        for offset in range(self.outer):
            self.inward(offset).wait_recv()
        for offset in range(1, self.outer):
            self.outward(offset).wait_send()
        for offset in range(self.outer):
            self.inward(offset).wait_send()


class Place:
    def __init__(self, outer):
        me, self.column = lax.axis_index("fs"), lax.axis_index("tp")
        self.me, self.low, self.outer = me, lax.rem(me, PAIR), outer
        self.z = me // PAIR
        self.near = self.z + 1 - 2 * lax.rem(self.z, 2)
        self.cross = outer - 1 - self.z
        self.skew = outer - 1 - self.near
        self.end = jnp.logical_or(self.z == 0, self.z == outer - 1)
        self.inner = jnp.logical_not(self.end)

    def same(self, z):
        return z * PAIR + self.low

    def other(self, z):
        return z * PAIR + 1 - self.low


class Spread:
    def __init__(self, place, view, span, send_sem, recv_sems, odd, own=None):
        self.place, self.view, self.span, self.odd = place, view, span, odd
        self.send_sem, self.recv_sems = send_sem, recv_sems
        self.own = view(place.me) if own is None else own

    def remote(self, src, dst, recv, target):
        return pltpu.make_async_remote_copy(
            src_ref=src,
            dst_ref=dst,
            send_sem=self.send_sem,
            recv_sem=self.recv_sems.at[recv],
            device_id=(target, self.place.column),
            device_id_type=MESH,
        )

    def mine(self, recv, target):
        return self.remote(self.own, self.view(self.place.me), recv, target)

    def passed(self, block, recv, target):
        return self.remote(self.view(block), self.view(block), recv, target)

    def to_skew(self):
        return self.mine(0, self.place.same(self.place.skew))

    def to_near(self):
        return self.mine(1, self.place.same(self.place.near))

    def to_cross(self):
        return self.mine(2, self.place.same(self.place.cross))

    def to_pair(self):
        return self.mine(3, self.place.other(self.place.z))

    def pair_on(self, z):
        return self.passed(self.place.same(z), 4, self.place.other(self.place.z))

    def relay_skew(self):
        return self.passed(self.place.same(self.place.skew), 2, self.place.same(self.place.near))

    def relay_pair(self):
        return self.passed(self.place.other(self.place.z), 4, self.place.same(self.place.near))

    def launch(self):
        self.launch_pair()
        self.launch_skew()
        self.launch_near()
        self.launch_cross()

    def launch_pair(self):
        self.to_pair().start()

    def launch_skew(self):
        self.to_skew().start()

    def launch_near(self):
        self.to_near().start()

    def launch_cross(self):
        pl.when(self.place.inner)(lambda: self.to_cross().start())

    def hop(self):
        self.to_skew().wait_recv()
        pl.when(self.place.inner)(lambda: self.relay_skew().start())

    def pass_skew(self):
        self.pair_on(self.place.skew).start()

    def pass_near(self):
        if not self.odd:
            self.to_near().wait_recv()
            pl.when(self.place.end)(lambda: self.pair_on(self.place.near).start())

    def pass_pair(self):
        self.to_pair().wait_recv()
        if self.odd:
            self.relay_pair().start()
        else:
            pl.when(self.place.end)(lambda: self.relay_pair().start())

    def pass_cross(self):
        self.to_cross().wait_recv()
        self.pair_on(self.place.cross).start()

    def relay(self):
        self.hop()
        self.pass_skew()
        self.pass_near()

    def many(self, count):
        return self.remote(self.span(count), self.span(count), 4, self.place.other(self.place.z))

    def collect(self):
        if self.odd:
            self.to_near().wait_recv()
        self.many(3).wait_recv()

    def drain(self):
        if self.odd:
            pl.when(self.place.end)(lambda: self.many(6).wait_send())
            pl.when(self.place.inner)(lambda: self.many(8).wait_send())
        else:
            self.many(7).wait_send()


def kernel(
    n_fs,
    n_tp,
    early_query,
    early_out,
    saved_hbm,
    outcot_hbm,
    querycot_hbm,
    attn_hbm,
    query_hbm,
    out_hbm,
    left_hbm,
    right_hbm,
    first_hbm,
    second_hbm,
    query_out,
    out_out,
    query_copy,
    out_copy,
    first_out,
    second_out,
    factor_ref,
    first_ref,
    second_ref,
    factors_ref,
    own_rows,
    dirs_ref,
    query_master,
    out_master,
    query_early,
    out_early,
    saved,
    outcot,
    querycot,
    attn,
    proj,
    grad,
    pair_send,
    pair_recv,
    far_send,
    far_recv,
    own_dir,
    square_buf,
    load_sems,
    rows_sems,
    proj_sems,
    columns_sems,
    pair_sems,
    far_sems,
    wire_sems,
    square_sems,
    spread_sends,
    spread_recvs,
):
    outer = n_fs // PAIR
    place = Place(outer)
    me, column, high, low = place.me, place.column, place.z, place.low
    part = factor_ref.shape[1]
    width = factor_ref.shape[2]
    depth = first_ref.shape[1]
    features = grad.shape[2]
    pieces = width // LANES
    tall, deep = LANES, features // pieces
    loads = [
        pltpu.make_async_copy(src, dst, load_sems.at[i])
        for i, (src, dst) in enumerate(
            (
                (saved_hbm, saved),
                (outcot_hbm, outcot),
                (querycot_hbm, querycot),
                (attn_hbm, attn),
                (query_hbm, query_master),
                (out_hbm, out_master),
                (first_hbm, first_ref),
                (second_hbm, second_ref),
                (left_hbm, factor_ref.at[0]),
                (right_hbm, factor_ref.at[1]),
            )
        )
    ]
    for load in loads[8:] + loads[:8]:
        load.start()

    fs_peers = [(lax.rem(me + i, n_fs), column) for i in range(1, n_fs)]
    tp_peers = [(me, lax.rem(column + i, n_tp)) for i in range(1, n_tp)]
    barrier = pltpu.get_barrier_semaphore()
    for peer in fs_peers + tp_peers:
        pl.semaphore_signal(barrier, inc=1, device_id=peer, device_id_type=MESH)
    for load in loads[8:]:
        load.wait()
    pl.semaphore_wait(barrier, len(fs_peers) + len(tp_peers))

    def spread(slot, view, span, odd, own=None):
        return Spread(place, view, span, spread_sends.at[slot], spread_recvs.at[slot], odd, own)

    factors = [
        spread(
            k,
            lambda i, k=k: factors_ref.at[k, rows(column, part), rows(i, width)],
            lambda n, k=k: factors_ref.at[k, :part, : n * width],
            k == 1,
            factor_ref.at[k],
        )
        for k in range(2)
    ]
    for gather in factors:
        gather.launch()
    own_columns = Gather("tp", n_tp, lambda i: own_rows.at[:, rows(i, part), :], rows_sems, own=factor_ref)
    own_columns.start()
    factors_ref[:, rows(column, part), rows(me, width)] = factor_ref[...]
    own_rows[:, rows(column, part), :] = factor_ref[...]

    def query_piece(i, own=None):
        return spread(
            4 + i,
            lambda j: query_copy.at[pl.ds(pl.multiple_of(j * width + i * tall, tall), tall), :],
            lambda n: query_copy.at[: n * tall, :],
            QUERY_ODD[i % 3],
            own,
        )

    def out_piece(i, own=None):
        return spread(
            4 + pieces + i,
            lambda j: out_copy.at[i * deep : (i + 1) * deep, rows(j, width)],
            lambda n: out_copy.at[:deep, : n * width],
            OUT_ODD[i % 3],
            own,
        )

    early_q = [query_piece(i, query_early.at[i]) for i in range(early_query)]
    early_o = [out_piece(i, out_early.at[i]) for i in range(early_out)]
    late_q = [query_piece(i) for i in range(early_query, pieces)]
    late_o = [out_piece(i) for i in range(early_out, pieces)]

    loads[4].wait()
    for i in range(early_query):
        query_early[i] = query_master[i * tall : (i + 1) * tall, :].astype(query_early.dtype)
    loads[5].wait()
    for i in range(early_out):
        out_early[i] = out_master[i * deep : (i + 1) * deep, :].astype(out_early.dtype)
    for gather in early_q:
        gather.launch_pair()
    for gather in factors:
        gather.relay()
    for gather in factors:
        gather.pass_pair()
    for gather in factors:
        gather.pass_cross()
    for gather in early_q:
        gather.launch_skew()
        gather.launch_near()
        gather.launch_cross()
    own_columns.forward()

    gathers = []
    for k, tokens in enumerate((saved, outcot)):
        factors[k].collect()
        loads[k].wait()
        part_proj = lax.dot_general(
            factors_ref[k, rows(column, part), :],
            tokens[...],
            NT,
            preferred_element_type=jnp.float32,
        )
        proj[k, rows(column, part), :] = part_proj.astype(proj.dtype)
        gather = Gather(
            "tp", n_tp, lambda i, k=k: proj.at[k, rows(i, part), :], proj_sems.at[k]
        )
        gather.start()
        gathers.append(gather)

    blocks = (place.cross, place.skew, place.near, place.z)

    def pair_copy(r, k):
        return pltpu.make_async_remote_copy(
            src_ref=pair_send.at[r, k],
            dst_ref=pair_recv.at[r, k],
            send_sem=wire_sems.at[0],
            recv_sem=pair_sems.at[r, k],
            device_id=(place.other(place.z), column),
            device_id_type=MESH,
        )

    def far_copy(r, k, slot, z):
        return pltpu.make_async_remote_copy(
            src_ref=far_send.at[r, k],
            dst_ref=far_recv.at[slot, k],
            send_sem=wire_sems.at[1],
            recv_sem=far_sems.at[slot, k],
            device_id=(place.same(z), column),
            device_id_type=MESH,
        )

    def both(r, k):
        return grad[k, rows(place.same(blocks[r]), depth), :] + pair_recv[r, k].astype(jnp.float32)

    columns = Gather("tp", n_tp, lambda i: factors_ref.at[:, rows(i, part), :], columns_sems)
    for k, (gather, cot) in enumerate(zip(gathers, (querycot, attn))):
        gather.forward()
        if k == 1:
            columns.start()
        gather.finish()
        loads[2 + k].wait()
        grad[k, :, :] = jnp.dot(proj[k], cot[...], preferred_element_type=jnp.float32)
        for r in range(outer):
            pair_send[r, k] = grad[k, rows(place.other(blocks[r]), depth), :].astype(pair_send.dtype)
            pair_copy(r, k).start()
    totals = []
    for k in range(2):
        for r in range(outer - 1):
            pair_copy(r, k).wait_recv()
            far_send[r, k] = both(r, k).astype(far_send.dtype)
            if r == outer - 2:
                far_copy(r, k, 2, place.near).start()
            else:
                pl.when(place.end)(lambda r=r, k=k: far_copy(r, k, 1 - r, place.near).start())
        pair_copy(outer - 1, k).wait_recv()
        totals.append(both(outer - 1, k))

        def add_near(k=k):
            for r in range(outer - 2):
                far_copy(r, k, r, place.near).wait_recv()
                far_send[r, k] = (both(r, k) + far_recv[r, k].astype(jnp.float32)).astype(far_send.dtype)
                far_copy(r, k, 3, blocks[r]).start()

        pl.when(place.inner)(add_near)
        if k == 0:
            for gather in early_q:
                gather.hop()
    for gather in early_q:
        gather.pass_skew()
    for k in range(2):
        for slot in (2, 3):
            far_copy(0, k, slot, place.near).wait_recv()
            totals[k] = totals[k] + far_recv[slot, k].astype(jnp.float32)

    shape = square_buf.shape[1:]
    row = lax.broadcasted_iota(jnp.int32, shape, 0)
    mine = jnp.zeros(shape, jnp.float32)
    for load in loads[6:8]:
        load.wait()
    for k in range(2):
        first_new, second_new, direction = moment_step(first_ref[k], second_ref[k], totals[k])
        own_dir[k] = direction.astype(own_dir.dtype)
        first_out[k] = first_new
        second_out[k] = second_new
        mine = jnp.where(row == k, jnp.sum(direction * direction), mine)

    def square_copy(base, slot, stage, count, target):
        return pltpu.make_async_remote_copy(
            src_ref=square_buf.at[pl.ds(base, count)],
            dst_ref=square_buf.at[pl.ds(slot, count)],
            send_sem=square_sems.at[stage, 0],
            recv_sem=square_sems.at[stage, 1],
            device_id=target,
            device_id_type=MESH,
        )

    def square_all(base, count, stage):
        return square_copy(base, base + 1, stage, count, tp_peers[0])

    square_buf[0] = mine
    for i, peer in enumerate(fs_peers):
        square_copy(0, 1 + i, 0, 1, peer).start()
    dirs = [
        spread(
            2 + k,
            lambda i, k=k: dirs_ref.at[k, rows(i, depth), :],
            lambda n, k=k: dirs_ref.at[k, : n * depth, :],
            k == 1,
            own_dir.at[k],
        )
        for k in range(2)
    ]
    for gather in dirs:
        gather.launch()
    dirs_ref[:, rows(me, depth), :] = own_dir[...]
    square_all(0, n_fs - 1, 0).wait_recv()
    mine = jnp.sum(square_buf[:n_fs], axis=0)
    square_buf[n_fs] = mine
    for i, peer in enumerate(tp_peers):
        square_copy(n_fs, n_fs + 1 + i, 1, 1, peer).start()
    for gather in dirs:
        gather.relay()
    for gather in dirs:
        gather.pass_pair()
    for gather in early_q:
        gather.pass_near()
        gather.pass_pair()
    for gather in early_o:
        gather.launch_skew()
        gather.launch_cross()
    for gather in dirs:
        gather.pass_cross()
    for gather in early_o:
        gather.launch_pair()
    square_all(n_fs, n_tp - 1, 1).wait_recv()
    mine = jnp.sum(square_buf[n_fs:], axis=0)
    entries = dirs_ref.shape[1] * dirs_ref.shape[2] * n_tp
    scale = 0.01 * lax.rsqrt(mine / entries + 1e-06)
    scales = (scale[0:1, 0:1], scale[1:2, 0:1])
    own_columns.finish()
    for gather in dirs:
        gather.collect()

    def launch_late(gathers):
        for gather in gathers:
            gather.launch_pair()
            gather.launch_skew()
            if not gather.odd:
                gather.launch_near()

    query_new = query_master[...] - scales[0] * lax.dot_general(
        own_rows[0], dirs_ref[0], TN, preferred_element_type=jnp.float32
    )
    query_out[...] = query_new
    query_copy[rows(me, width), :] = query_new.astype(query_copy.dtype)
    launch_late(late_q)
    out_new = out_master[...] - scales[1] * lax.dot_general(
        dirs_ref[1], own_rows[1], TN, preferred_element_type=jnp.float32
    )
    out_out[...] = out_new
    out_copy[:, rows(me, width)] = out_new.astype(out_copy.dtype)
    launch_late(late_o)
    for gather in late_q + late_o:
        gather.launch_cross()

    columns.forward()
    bulk = early_o + late_q + late_o

    def finish_near(gather):
        if gather.odd:
            gather.launch_near()
        gather.pass_pair()

    crossing = early_q + bulk
    for i, gather in enumerate(bulk):
        gather.relay()
        if i >= 1:
            pl.when(place.end)(crossing[i + 1 - 2].pass_cross)
        if i >= 3:
            finish_near(bulk[i - 3])
    for gather in bulk[max(len(bulk) - 3, 0) :]:
        finish_near(gather)
    for gather in crossing[:-2]:
        pl.when(place.inner)(gather.pass_cross)
    for gather in crossing[-2:]:
        gather.pass_cross()
    columns.finish()

    for gather in early_q + early_o:
        gather.collect()
        gather.drain()

    def finish_block(i, carry):
        block = lax.rem(me + i, n_fs)
        for j in range(early_query):
            where = pl.ds(pl.multiple_of(block * width + j * tall, tall), tall)
            step = lax.dot_general(
                factors_ref[0, :, where], dirs_ref[0], TN, preferred_element_type=jnp.float32
            )
            query = query_copy[where, :].astype(jnp.float32)
            query_copy[where, :] = (query - scales[0] * step).astype(query_copy.dtype)
        for j in range(early_out):
            band = slice(j * deep, (j + 1) * deep)
            step = lax.dot_general(
                dirs_ref[1, :, band],
                factors_ref[1, :, rows(block, width)],
                TN,
                preferred_element_type=jnp.float32,
            )
            out = out_copy[band, rows(block, width)].astype(jnp.float32)
            out_copy[band, rows(block, width)] = (out - scales[1] * step).astype(out_copy.dtype)
        return carry

    lax.fori_loop(1, n_fs, finish_block, 0)
    for gather in late_q + late_o:
        gather.collect()
    for gather in factors + dirs + late_q + late_o:
        gather.drain()
    pltpu.make_async_copy(pair_send, pair_recv, wire_sems.at[0]).wait()
    pltpu.make_async_copy(far_send.at[1:], far_send.at[1:], wire_sems.at[1]).wait()
    square_all(0, n_fs - 1, 0).wait_send()
    square_all(n_fs, n_tp - 1, 1).wait_send()


def store_kernel(*refs):
    count = len(refs) // 2
    sems = refs[-1]
    copies = []
    for i in range(count):
        size = refs[i].shape[0] // STORES if refs[i].shape[0] % (16 * STORES) == 0 else refs[i].shape[0]
        for j in range(refs[i].shape[0] // size):
            band = slice(j * size, (j + 1) * size)
            copies.append(pltpu.make_async_copy(refs[i].at[band], refs[count + i].at[band], sems.at[i, j]))
    for copy in copies:
        copy.start()
    for copy in copies:
        copy.wait()


def fast_body(
    n_fs,
    n_tp,
    saved_inputs,
    query_cotangent,
    attn_outputs,
    out_cotangent,
    left_factor,
    right_factor,
    query_master,
    out_master,
    first_moment,
    second_moment,
):
    tokens, model = saved_inputs.shape
    features = query_cotangent.shape[1]
    width, part = left_factor.shape
    depth = first_moment.shape[1]
    rank = part * n_tp
    outer = n_fs // PAIR
    pieces = width // LANES
    low, wide = jnp.bfloat16, jnp.float32
    vmem = pl.BlockSpec(memory_space=pltpu.VMEM)
    anywhere = pl.BlockSpec(memory_space=pl.ANY)
    dma = pltpu.SemaphoreType.DMA
    results = pl.pallas_call(
        functools.partial(kernel, n_fs, n_tp, EARLY_QUERY, EARLY_OUT),
        out_shape=(
            pltpu.VMEM((width, features), wide),
            pltpu.VMEM((features, width), wide),
            pltpu.VMEM((model, features), low),
            pltpu.VMEM((features, model), low),
            pltpu.VMEM(first_moment.shape, wide),
            pltpu.VMEM(first_moment.shape, wide),
        ),
        in_specs=[anywhere] * 10,
        out_specs=(vmem,) * 6,
        scratch_shapes=[
            pltpu.VMEM((2, part, width), low),
            pltpu.VMEM(first_moment.shape, wide),
            pltpu.VMEM(first_moment.shape, wide),
            pltpu.VMEM((2, rank, model), low),
            pltpu.VMEM((2, rank, width), low),
            pltpu.VMEM((2, rank, features), low),
            pltpu.VMEM((width, features), wide),
            pltpu.VMEM((features, width), wide),
            pltpu.VMEM((max(EARLY_QUERY, 1), LANES, features), low),
            pltpu.VMEM((max(EARLY_OUT, 1), features // pieces, width), low),
            pltpu.VMEM((tokens, model), low),
            pltpu.VMEM((tokens, model), low),
            pltpu.VMEM((tokens, features), low),
            pltpu.VMEM((tokens, features), low),
            pltpu.VMEM((2, rank, tokens), low),
            pltpu.VMEM((2, rank, features), wide),
            pltpu.VMEM((outer, 2, depth, features), low),
            pltpu.VMEM((outer, 2, depth, features), low),
            pltpu.VMEM((outer, 2, depth, features), low),
            pltpu.VMEM((outer, 2, depth, features), low),
            pltpu.VMEM((2, depth, features), low),
            pltpu.VMEM((n_fs + n_tp, 8, 128), wide),
            dma((10,)),
            dma((2, 2, n_tp // PAIR)),
            dma((2, 2, 2, n_tp // PAIR)),
            dma((2, 2, n_tp // PAIR)),
            dma((outer, 2)),
            dma((outer, 2)),
            dma((2,)),
            dma((2, 2)),
            dma((4 + 2 * pieces,)),
            dma((4 + 2 * pieces, 5)),
        ],
        compiler_params=pltpu.CompilerParams(
            collective_id=0, has_side_effects=True, vmem_limit_bytes=46 * 2**20
        ),
        cost_estimate=pl.CostEstimate(
            flops=4 * tokens * rank * (model + features), bytes_accessed=200 * 2**20, transcendentals=0
        ),
    )(
        saved_inputs,
        out_cotangent,
        query_cotangent,
        attn_outputs,
        query_master,
        out_master,
        left_factor.T,
        right_factor.T,
        first_moment,
        second_moment,
    )
    return pl.pallas_call(
        store_kernel,
        out_shape=tuple(jax.ShapeDtypeStruct(r.shape, r.dtype) for r in results),
        in_specs=[vmem] * len(results),
        out_specs=(anywhere,) * len(results),
        scratch_shapes=[dma((len(results), STORES))],
        compiler_params=pltpu.CompilerParams(vmem_limit_bytes=2**20),
        cost_estimate=pl.CostEstimate(flops=2**20, bytes_accessed=13 * 2**20, transcendentals=0),
    )(*(pltpu.with_memory_space_constraint(r, pltpu.VMEM) for r in results))


def plain_body(
    saved_inputs,
    query_cotangent,
    attn_outputs,
    out_cotangent,
    left_factor,
    right_factor,
    query_master,
    out_master,
    first_moment,
    second_moment,
):
    left_part = jnp.dot(
        saved_inputs,
        lax.all_gather(left_factor, "fs", axis=0, tiled=True),
        preferred_element_type=jnp.float32,
    )
    right_part = jnp.dot(
        out_cotangent,
        lax.all_gather(right_factor, "fs", axis=0, tiled=True),
        preferred_element_type=jnp.float32,
    )
    left_proj, right_proj, left_rows, right_rows = (
        lax.all_gather(left_part.astype(jnp.bfloat16), "tp", axis=1, tiled=True),
        lax.all_gather(right_part.astype(jnp.bfloat16), "tp", axis=1, tiled=True),
        lax.all_gather(left_factor, "tp", axis=1, tiled=True),
        lax.all_gather(right_factor, "tp", axis=1, tiled=True),
    )
    depth = first_moment.shape[1]
    grad_query = lax.dot_general(left_proj, query_cotangent, TN, preferred_element_type=jnp.float32)
    grad_output = lax.dot_general(right_proj, attn_outputs, TN, preferred_element_type=jnp.float32)
    summed = lax.psum_scatter(
        jnp.stack([grad_query, grad_output], axis=1), "fs", scatter_dimension=0, tiled=True
    )
    grads = jnp.transpose(summed, (1, 0, 2))
    first_new, second_new, own_direction = moment_step(first_moment, second_moment, grads)
    direction_all = lax.all_gather(own_direction.astype(jnp.bfloat16), "fs", axis=1, tiled=True)
    squares = jnp.sum(own_direction * own_direction, axis=(1, 2))
    total = lax.psum(squares, ("fs", "tp"))
    entries = depth * lax.axis_size("fs") * own_direction.shape[2] * lax.axis_size("tp")
    scale = lax.rsqrt(total / entries + 1e-06)
    step_query = scale[0] * jnp.dot(left_rows, direction_all[0], preferred_element_type=jnp.float32)
    step_output = scale[1] * lax.dot_general(
        direction_all[1], right_rows, (((0,), (1,)), ((), ())), preferred_element_type=jnp.float32
    )
    query_new = query_master - 0.01 * step_query
    out_new = out_master - 0.01 * step_output
    query_copy, out_copy = (
        lax.all_gather(query_new.astype(jnp.bfloat16), "fs", axis=0, tiled=True),
        lax.all_gather(out_new.astype(jnp.bfloat16), "fs", axis=1, tiled=True),
    )
    return (query_new, out_new, query_copy, out_copy, first_new, second_new)


def choose_body(n_fs, n_tp, *args):
    left_factor, first_moment = args[4], args[8]
    model, part = args[0].shape[1], left_factor.shape[1]
    aligned = part % 16 == 0 and first_moment.shape[1] % 16 == 0
    aligned = aligned and model // n_fs % 128 == 0 and first_moment.shape[2] % 256 == 0
    aligned = aligned and first_moment.shape[2] % (model // n_fs) == 0
    if aligned and n_fs == PAIR * LINE and n_tp % PAIR == 0:
        return fast_body(n_fs, n_tp, *args)
    return plain_body(*args)


def solution(mesh):
    return jax.shard_map(
        functools.partial(choose_body, mesh.shape["fs"], mesh.shape["tp"]),
        mesh=mesh,
        in_specs=(
            P("fs", None),
            P("fs", "tp"),
            P("fs", "tp"),
            P("fs", None),
            P("fs", "tp"),
            P("fs", "tp"),
            P("fs", "tp"),
            P("tp", "fs"),
            P(None, "fs", "tp"),
            P(None, "fs", "tp"),
        ),
        out_specs=(
            P("fs", "tp"),
            P("tp", "fs"),
            P(None, "tp"),
            P("tp", None),
            P(None, "fs", "tp"),
            P(None, "fs", "tp"),
        ),
        check_vma=False,
    )
```

```python
import functools

import jax
import jax.numpy as jnp
from jax import lax
from jax.experimental import pallas as pl
from jax.experimental.pallas import tpu as pltpu
from jax.sharding import PartitionSpec as P

MESH = pl.DeviceIdType.MESH
PAIR = 2
LINE = 4
LANES = 128
EARLY_QUERY = 1
EARLY_OUT = 1
STORES = 4
QUERY_ODD = (True, False, True)
OUT_ODD = (True, False, True)
NT = (((1,), (1,)), ((), ()))
TN = (((0,), (0,)), ((), ()))


def moment_step(first, second, grads):
    first_next = 0.9 * first + 0.1 * grads
    second_next = 0.99 * second + 0.01 * grads * grads
    return (first_next, second_next, first_next / (jnp.sqrt(second_next) + 1e-08))


def rows(index, size):
    return pl.ds(pl.multiple_of(index * size, size), size)


def peer_along(axis, index):
    if axis == "fs":
        return (index, lax.axis_index("tp"))
    return (lax.axis_index("fs"), index)


class Gather:
    def __init__(self, axis, count, view, sems, own=None):
        self.axis, self.outer, self.view, self.sems = axis, count // PAIR, view, sems
        me = lax.axis_index(axis)
        self.high, self.low = me // PAIR, lax.rem(me, PAIR)
        self.own = view(me) if own is None else own
        self.me = me

    def copy(self, src, dst, stage, slot, target):
        return pltpu.make_async_remote_copy(
            src_ref=src,
            dst_ref=dst,
            send_sem=self.sems.at[stage, 0, slot],
            recv_sem=self.sems.at[stage, 1, slot],
            device_id=peer_along(self.axis, target),
            device_id_type=MESH,
        )

    def index(self, offset, low):
        return lax.rem(self.high + offset, self.outer) * PAIR + low

    def outward(self, offset):
        return self.copy(self.own, self.view(self.me), 0, offset, self.index(offset, self.low))

    def inward(self, offset):
        source = self.index(self.outer - offset, self.low)
        src = self.own if offset == 0 else self.view(source)
        partner = self.high * PAIR + 1 - self.low
        return self.copy(src, self.view(self.me if offset == 0 else source), 1, offset, partner)

    def start_outward(self):
        for offset in range(self.outer - 1, 0, -1):
            self.outward(offset).start()

    def start_inward(self):
        self.inward(0).start()

    def start(self):
        self.start_outward()
        self.start_inward()

    def forward(self):
        for offset in range(self.outer - 1, 0, -1):
            self.outward(offset).wait_recv()
            self.inward(offset).start()

    def finish(self):
        for offset in range(self.outer):
            self.inward(offset).wait_recv()
        for offset in range(1, self.outer):
            self.outward(offset).wait_send()
        for offset in range(self.outer):
            self.inward(offset).wait_send()


class Place:
    def __init__(self, outer):
        me, self.column = lax.axis_index("fs"), lax.axis_index("tp")
        self.me, self.low, self.outer = me, lax.rem(me, PAIR), outer
        self.z = me // PAIR
        self.near = self.z + 1 - 2 * lax.rem(self.z, 2)
        self.cross = outer - 1 - self.z
        self.skew = outer - 1 - self.near
        self.end = jnp.logical_or(self.z == 0, self.z == outer - 1)
        self.inner = jnp.logical_not(self.end)

    def same(self, z):
        return z * PAIR + self.low

    def other(self, z):
        return z * PAIR + 1 - self.low


class Spread:
    def __init__(self, place, view, span, send_sem, recv_sems, odd, own=None):
        self.place, self.view, self.span, self.odd = place, view, span, odd
        self.send_sem, self.recv_sems = send_sem, recv_sems
        self.own = view(place.me) if own is None else own

    def remote(self, src, dst, recv, target):
        return pltpu.make_async_remote_copy(
            src_ref=src,
            dst_ref=dst,
            send_sem=self.send_sem,
            recv_sem=self.recv_sems.at[recv],
            device_id=(target, self.place.column),
            device_id_type=MESH,
        )

    def mine(self, recv, target):
        return self.remote(self.own, self.view(self.place.me), recv, target)

    def passed(self, block, recv, target):
        return self.remote(self.view(block), self.view(block), recv, target)

    def to_skew(self):
        return self.mine(0, self.place.same(self.place.skew))

    def to_near(self):
        return self.mine(1, self.place.same(self.place.near))

    def to_cross(self):
        return self.mine(2, self.place.same(self.place.cross))

    def to_pair(self):
        return self.mine(3, self.place.other(self.place.z))

    def pair_on(self, z):
        return self.passed(self.place.same(z), 4, self.place.other(self.place.z))

    def relay_skew(self):
        return self.passed(self.place.same(self.place.skew), 2, self.place.same(self.place.near))

    def relay_pair(self):
        return self.passed(self.place.other(self.place.z), 4, self.place.same(self.place.near))

    def launch(self):
        self.launch_pair()
        self.launch_skew()
        self.launch_near()
        self.launch_cross()

    def launch_pair(self):
        self.to_pair().start()

    def launch_skew(self):
        self.to_skew().start()

    def launch_near(self):
        self.to_near().start()

    def launch_cross(self):
        pl.when(self.place.inner)(lambda: self.to_cross().start())

    def hop(self):
        self.to_skew().wait_recv()
        pl.when(self.place.inner)(lambda: self.relay_skew().start())

    def pass_skew(self):
        self.pair_on(self.place.skew).start()

    def pass_near(self):
        if not self.odd:
            self.to_near().wait_recv()
            pl.when(self.place.end)(lambda: self.pair_on(self.place.near).start())

    def pass_pair(self):
        self.to_pair().wait_recv()
        if self.odd:
            self.relay_pair().start()
        else:
            pl.when(self.place.end)(lambda: self.relay_pair().start())

    def pass_cross(self):
        self.to_cross().wait_recv()
        self.pair_on(self.place.cross).start()

    def relay(self):
        self.hop()
        self.pass_skew()
        self.pass_near()

    def many(self, count):
        return self.remote(self.span(count), self.span(count), 4, self.place.other(self.place.z))

    def collect(self):
        if self.odd:
            self.to_near().wait_recv()
        self.many(3).wait_recv()

    def drain(self):
        if self.odd:
            pl.when(self.place.end)(lambda: self.many(6).wait_send())
            pl.when(self.place.inner)(lambda: self.many(8).wait_send())
        else:
            self.many(7).wait_send()


def kernel(
    n_fs,
    n_tp,
    early_query,
    early_out,
    saved_hbm,
    outcot_hbm,
    querycot_hbm,
    attn_hbm,
    query_hbm,
    out_hbm,
    left_hbm,
    right_hbm,
    first_hbm,
    second_hbm,
    query_out,
    out_out,
    query_copy,
    out_copy,
    first_out,
    second_out,
    factor_ref,
    first_ref,
    second_ref,
    factors_ref,
    own_rows,
    dirs_ref,
    query_master,
    out_master,
    query_early,
    out_early,
    saved,
    outcot,
    querycot,
    attn,
    proj,
    grad,
    pair_send,
    pair_recv,
    far_send,
    far_recv,
    own_dir,
    square_buf,
    load_sems,
    rows_sems,
    proj_sems,
    columns_sems,
    pair_sems,
    far_sems,
    wire_sems,
    square_sems,
    spread_sends,
    spread_recvs,
):
    outer = n_fs // PAIR
    place = Place(outer)
    me, column, high, low = place.me, place.column, place.z, place.low
    part = factor_ref.shape[1]
    width = factor_ref.shape[2]
    depth = first_ref.shape[1]
    features = grad.shape[2]
    pieces = width // LANES
    tall, deep = LANES, features // pieces
    loads = [
        pltpu.make_async_copy(src, dst, load_sems.at[i])
        for i, (src, dst) in enumerate(
            (
                (saved_hbm, saved),
                (outcot_hbm, outcot),
                (querycot_hbm, querycot),
                (attn_hbm, attn),
                (query_hbm, query_master),
                (out_hbm, out_master),
                (first_hbm, first_ref),
                (second_hbm, second_ref),
                (left_hbm, factor_ref.at[0]),
                (right_hbm, factor_ref.at[1]),
            )
        )
    ]
    for load in loads[8:] + loads[:8]:
        load.start()

    fs_peers = [(lax.rem(me + i, n_fs), column) for i in range(1, n_fs)]
    tp_peers = [(me, lax.rem(column + i, n_tp)) for i in range(1, n_tp)]
    barrier = pltpu.get_barrier_semaphore()
    for peer in fs_peers + tp_peers:
        pl.semaphore_signal(barrier, inc=1, device_id=peer, device_id_type=MESH)
    for load in loads[8:]:
        load.wait()
    pl.semaphore_wait(barrier, len(fs_peers) + len(tp_peers))

    def spread(slot, view, span, odd, own=None):
        return Spread(place, view, span, spread_sends.at[slot], spread_recvs.at[slot], odd, own)

    factors = [
        spread(
            k,
            lambda i, k=k: factors_ref.at[k, rows(column, part), rows(i, width)],
            lambda n, k=k: factors_ref.at[k, :part, : n * width],
            k == 1,
            factor_ref.at[k],
        )
        for k in range(2)
    ]
    for gather in factors:
        gather.launch()
    own_columns = Gather("tp", n_tp, lambda i: own_rows.at[:, rows(i, part), :], rows_sems, own=factor_ref)
    own_columns.start()
    factors_ref[:, rows(column, part), rows(me, width)] = factor_ref[...]
    own_rows[:, rows(column, part), :] = factor_ref[...]

    def query_piece(i, own=None):
        return spread(
            4 + i,
            lambda j: query_copy.at[pl.ds(pl.multiple_of(j * width + i * tall, tall), tall), :],
            lambda n: query_copy.at[: n * tall, :],
            QUERY_ODD[i % 3],
            own,
        )

    def out_piece(i, own=None):
        return spread(
            4 + pieces + i,
            lambda j: out_copy.at[i * deep : (i + 1) * deep, rows(j, width)],
            lambda n: out_copy.at[:deep, : n * width],
            OUT_ODD[i % 3],
            own,
        )

    early_q = [query_piece(i, query_early.at[i]) for i in range(early_query)]
    early_o = [out_piece(i, out_early.at[i]) for i in range(early_out)]
    late_q = [query_piece(i) for i in range(early_query, pieces)]
    late_o = [out_piece(i) for i in range(early_out, pieces)]

    loads[4].wait()
    for i in range(early_query):
        query_early[i] = query_master[i * tall : (i + 1) * tall, :].astype(query_early.dtype)
    loads[5].wait()
    for i in range(early_out):
        out_early[i] = out_master[i * deep : (i + 1) * deep, :].astype(out_early.dtype)
    for gather in early_q:
        gather.launch_pair()
    for gather in factors:
        gather.relay()
    for gather in factors:
        gather.pass_pair()
    for gather in factors:
        gather.pass_cross()
    for gather in early_q:
        gather.launch_skew()
        gather.launch_near()
        gather.launch_cross()
    for gather in early_o:
        gather.launch_pair()
        gather.launch_near()
    own_columns.forward()

    gathers = []
    for k, tokens in enumerate((saved, outcot)):
        factors[k].collect()
        loads[k].wait()
        part_proj = lax.dot_general(
            factors_ref[k, rows(column, part), :],
            tokens[...],
            NT,
            preferred_element_type=jnp.float32,
        )
        proj[k, rows(column, part), :] = part_proj.astype(proj.dtype)
        gather = Gather(
            "tp", n_tp, lambda i, k=k: proj.at[k, rows(i, part), :], proj_sems.at[k]
        )
        gather.start()
        gathers.append(gather)

    blocks = (place.cross, place.skew, place.near, place.z)

    def pair_copy(r, k):
        return pltpu.make_async_remote_copy(
            src_ref=pair_send.at[r, k],
            dst_ref=pair_recv.at[r, k],
            send_sem=wire_sems.at[0],
            recv_sem=pair_sems.at[r, k],
            device_id=(place.other(place.z), column),
            device_id_type=MESH,
        )

    def far_copy(r, k, slot, z):
        return pltpu.make_async_remote_copy(
            src_ref=far_send.at[r, k],
            dst_ref=far_recv.at[slot, k],
            send_sem=wire_sems.at[1],
            recv_sem=far_sems.at[slot, k],
            device_id=(place.same(z), column),
            device_id_type=MESH,
        )

    def both(r, k):
        return grad[k, rows(place.same(blocks[r]), depth), :] + pair_recv[r, k].astype(jnp.float32)

    columns = Gather("tp", n_tp, lambda i: factors_ref.at[:, rows(i, part), :], columns_sems)
    for k, (gather, cot) in enumerate(zip(gathers, (querycot, attn))):
        gather.forward()
        if k == 1:
            columns.start()
        gather.finish()
        loads[2 + k].wait()
        grad[k, :, :] = jnp.dot(proj[k], cot[...], preferred_element_type=jnp.float32)
        for r in range(outer):
            pair_send[r, k] = grad[k, rows(place.other(blocks[r]), depth), :].astype(pair_send.dtype)
            pair_copy(r, k).start()
    totals = []
    for k in range(2):
        for r in range(outer - 1):
            pair_copy(r, k).wait_recv()
            far_send[r, k] = both(r, k).astype(far_send.dtype)
            if r == outer - 2:
                far_copy(r, k, 2, place.near).start()
            else:
                pl.when(place.end)(lambda r=r, k=k: far_copy(r, k, 1 - r, place.near).start())
        pair_copy(outer - 1, k).wait_recv()
        totals.append(both(outer - 1, k))

        def add_near(k=k):
            for r in range(outer - 2):
                far_copy(r, k, r, place.near).wait_recv()
                far_send[r, k] = (both(r, k) + far_recv[r, k].astype(jnp.float32)).astype(far_send.dtype)
                far_copy(r, k, 3, blocks[r]).start()

        pl.when(place.inner)(add_near)
        if k == 0:
            for gather in early_q:
                gather.hop()
    for gather in early_q:
        gather.pass_skew()
    for k in range(2):
        for slot in (2, 3):
            far_copy(0, k, slot, place.near).wait_recv()
            totals[k] = totals[k] + far_recv[slot, k].astype(jnp.float32)

    shape = square_buf.shape[1:]
    row = lax.broadcasted_iota(jnp.int32, shape, 0)
    mine = jnp.zeros(shape, jnp.float32)
    for load in loads[6:8]:
        load.wait()
    for k in range(2):
        first_new, second_new, direction = moment_step(first_ref[k], second_ref[k], totals[k])
        own_dir[k] = direction.astype(own_dir.dtype)
        first_out[k] = first_new
        second_out[k] = second_new
        mine = jnp.where(row == k, jnp.sum(direction * direction), mine)

    def square_copy(base, slot, stage, count, target):
        return pltpu.make_async_remote_copy(
            src_ref=square_buf.at[pl.ds(base, count)],
            dst_ref=square_buf.at[pl.ds(slot, count)],
            send_sem=square_sems.at[stage, 0],
            recv_sem=square_sems.at[stage, 1],
            device_id=target,
            device_id_type=MESH,
        )

    def square_all(base, count, stage):
        return square_copy(base, base + 1, stage, count, tp_peers[0])

    square_buf[0] = mine
    for i, peer in enumerate(fs_peers):
        square_copy(0, 1 + i, 0, 1, peer).start()
    dirs = [
        spread(
            2 + k,
            lambda i, k=k: dirs_ref.at[k, rows(i, depth), :],
            lambda n, k=k: dirs_ref.at[k, : n * depth, :],
            k == 1,
            own_dir.at[k],
        )
        for k in range(2)
    ]
    for gather in dirs:
        gather.launch()
    dirs_ref[:, rows(me, depth), :] = own_dir[...]
    for gather in dirs:
        gather.relay()
    for gather in dirs:
        gather.pass_pair()
    for gather in early_q:
        gather.pass_near()
        gather.pass_pair()
    for gather in early_o:
        gather.pass_pair()
    for gather in early_o:
        gather.launch_skew()
        gather.launch_cross()
    square_all(0, n_fs - 1, 0).wait_recv()
    mine = jnp.sum(square_buf[:n_fs], axis=0)
    square_buf[n_fs] = mine
    for i, peer in enumerate(tp_peers):
        square_copy(n_fs, n_fs + 1 + i, 1, 1, peer).start()
    for gather in dirs:
        gather.pass_cross()
    square_all(n_fs, n_tp - 1, 1).wait_recv()
    mine = jnp.sum(square_buf[n_fs:], axis=0)
    entries = dirs_ref.shape[1] * dirs_ref.shape[2] * n_tp
    scale = 0.01 * lax.rsqrt(mine / entries + 1e-06)
    scales = (scale[0:1, 0:1], scale[1:2, 0:1])
    own_columns.finish()
    for gather in dirs:
        gather.collect()

    def launch_late(gathers):
        for gather in gathers:
            gather.launch_pair()
            gather.launch_skew()
            if not gather.odd:
                gather.launch_near()

    query_new = query_master[...] - scales[0] * lax.dot_general(
        own_rows[0], dirs_ref[0], TN, preferred_element_type=jnp.float32
    )
    query_out[...] = query_new
    query_copy[rows(me, width), :] = query_new.astype(query_copy.dtype)
    launch_late(late_q)
    out_new = out_master[...] - scales[1] * lax.dot_general(
        dirs_ref[1], own_rows[1], TN, preferred_element_type=jnp.float32
    )
    out_out[...] = out_new
    out_copy[:, rows(me, width)] = out_new.astype(out_copy.dtype)
    launch_late(late_o)
    for gather in late_q + late_o:
        gather.launch_cross()

    columns.forward()
    bulk = early_o + late_q + late_o

    def finish_near(gather):
        if gather not in early_o:
            if gather.odd:
                gather.launch_near()
            gather.pass_pair()

    crossing = early_q + bulk
    for i, gather in enumerate(bulk):
        gather.relay()
        if i >= 1:
            pl.when(place.end)(crossing[i + 1 - 2].pass_cross)
        if i >= 9:
            finish_near(bulk[i - 9])
    for gather in bulk[max(len(bulk) - 9, 0) :]:
        finish_near(gather)
    for gather in crossing[:-2]:
        pl.when(place.inner)(gather.pass_cross)
    for gather in crossing[-2:]:
        gather.pass_cross()
    columns.finish()

    for gather in early_q + early_o:
        gather.collect()
        gather.drain()

    def finish_block(i, carry):
        block = lax.rem(me + i, n_fs)
        for j in range(early_query):
            where = pl.ds(pl.multiple_of(block * width + j * tall, tall), tall)
            step = lax.dot_general(
                factors_ref[0, :, where], dirs_ref[0], TN, preferred_element_type=jnp.float32
            )
            query = query_copy[where, :].astype(jnp.float32)
            query_copy[where, :] = (query - scales[0] * step).astype(query_copy.dtype)
        for j in range(early_out):
            band = slice(j * deep, (j + 1) * deep)
            step = lax.dot_general(
                dirs_ref[1, :, band],
                factors_ref[1, :, rows(block, width)],
                TN,
                preferred_element_type=jnp.float32,
            )
            out = out_copy[band, rows(block, width)].astype(jnp.float32)
            out_copy[band, rows(block, width)] = (out - scales[1] * step).astype(out_copy.dtype)
        return carry

    lax.fori_loop(1, n_fs, finish_block, 0)
    for gather in late_q + late_o:
        gather.collect()
    for gather in factors + dirs + late_q + late_o:
        gather.drain()
    pltpu.make_async_copy(pair_send, pair_recv, wire_sems.at[0]).wait()
    pltpu.make_async_copy(far_send.at[1:], far_send.at[1:], wire_sems.at[1]).wait()
    square_all(0, n_fs - 1, 0).wait_send()
    square_all(n_fs, n_tp - 1, 1).wait_send()


def store_kernel(*refs):
    count = len(refs) // 2
    sems = refs[-1]
    copies = []
    for i in range(count):
        size = refs[i].shape[0] // STORES if refs[i].shape[0] % (16 * STORES) == 0 else refs[i].shape[0]
        for j in range(refs[i].shape[0] // size):
            band = slice(j * size, (j + 1) * size)
            copies.append(pltpu.make_async_copy(refs[i].at[band], refs[count + i].at[band], sems.at[i, j]))
    for copy in copies:
        copy.start()
    for copy in copies:
        copy.wait()


def fast_body(
    n_fs,
    n_tp,
    saved_inputs,
    query_cotangent,
    attn_outputs,
    out_cotangent,
    left_factor,
    right_factor,
    query_master,
    out_master,
    first_moment,
    second_moment,
):
    tokens, model = saved_inputs.shape
    features = query_cotangent.shape[1]
    width, part = left_factor.shape
    depth = first_moment.shape[1]
    rank = part * n_tp
    outer = n_fs // PAIR
    pieces = width // LANES
    low, wide = jnp.bfloat16, jnp.float32
    vmem = pl.BlockSpec(memory_space=pltpu.VMEM)
    anywhere = pl.BlockSpec(memory_space=pl.ANY)
    dma = pltpu.SemaphoreType.DMA
    results = pl.pallas_call(
        functools.partial(kernel, n_fs, n_tp, EARLY_QUERY, EARLY_OUT),
        out_shape=(
            pltpu.VMEM((width, features), wide),
            pltpu.VMEM((features, width), wide),
            pltpu.VMEM((model, features), low),
            pltpu.VMEM((features, model), low),
            pltpu.VMEM(first_moment.shape, wide),
            pltpu.VMEM(first_moment.shape, wide),
        ),
        in_specs=[anywhere] * 10,
        out_specs=(vmem,) * 6,
        scratch_shapes=[
            pltpu.VMEM((2, part, width), low),
            pltpu.VMEM(first_moment.shape, wide),
            pltpu.VMEM(first_moment.shape, wide),
            pltpu.VMEM((2, rank, model), low),
            pltpu.VMEM((2, rank, width), low),
            pltpu.VMEM((2, rank, features), low),
            pltpu.VMEM((width, features), wide),
            pltpu.VMEM((features, width), wide),
            pltpu.VMEM((max(EARLY_QUERY, 1), LANES, features), low),
            pltpu.VMEM((max(EARLY_OUT, 1), features // pieces, width), low),
            pltpu.VMEM((tokens, model), low),
            pltpu.VMEM((tokens, model), low),
            pltpu.VMEM((tokens, features), low),
            pltpu.VMEM((tokens, features), low),
            pltpu.VMEM((2, rank, tokens), low),
            pltpu.VMEM((2, rank, features), wide),
            pltpu.VMEM((outer, 2, depth, features), low),
            pltpu.VMEM((outer, 2, depth, features), low),
            pltpu.VMEM((outer, 2, depth, features), low),
            pltpu.VMEM((outer, 2, depth, features), low),
            pltpu.VMEM((2, depth, features), low),
            pltpu.VMEM((n_fs + n_tp, 8, 128), wide),
            dma((10,)),
            dma((2, 2, n_tp // PAIR)),
            dma((2, 2, 2, n_tp // PAIR)),
            dma((2, 2, n_tp // PAIR)),
            dma((outer, 2)),
            dma((outer, 2)),
            dma((2,)),
            dma((2, 2)),
            dma((4 + 2 * pieces,)),
            dma((4 + 2 * pieces, 5)),
        ],
        compiler_params=pltpu.CompilerParams(
            collective_id=0, has_side_effects=True, vmem_limit_bytes=46 * 2**20
        ),
        cost_estimate=pl.CostEstimate(
            flops=4 * tokens * rank * (model + features), bytes_accessed=200 * 2**20, transcendentals=0
        ),
    )(
        saved_inputs,
        out_cotangent,
        query_cotangent,
        attn_outputs,
        query_master,
        out_master,
        left_factor.T,
        right_factor.T,
        first_moment,
        second_moment,
    )
    return pl.pallas_call(
        store_kernel,
        out_shape=tuple(jax.ShapeDtypeStruct(r.shape, r.dtype) for r in results),
        in_specs=[vmem] * len(results),
        out_specs=(anywhere,) * len(results),
        scratch_shapes=[dma((len(results), STORES))],
        compiler_params=pltpu.CompilerParams(vmem_limit_bytes=2**20),
        cost_estimate=pl.CostEstimate(flops=2**20, bytes_accessed=13 * 2**20, transcendentals=0),
    )(*(pltpu.with_memory_space_constraint(r, pltpu.VMEM) for r in results))


def plain_body(
    saved_inputs,
    query_cotangent,
    attn_outputs,
    out_cotangent,
    left_factor,
    right_factor,
    query_master,
    out_master,
    first_moment,
    second_moment,
):
    left_part = jnp.dot(
        saved_inputs,
        lax.all_gather(left_factor, "fs", axis=0, tiled=True),
        preferred_element_type=jnp.float32,
    )
    right_part = jnp.dot(
        out_cotangent,
        lax.all_gather(right_factor, "fs", axis=0, tiled=True),
        preferred_element_type=jnp.float32,
    )
    left_proj, right_proj, left_rows, right_rows = (
        lax.all_gather(left_part.astype(jnp.bfloat16), "tp", axis=1, tiled=True),
        lax.all_gather(right_part.astype(jnp.bfloat16), "tp", axis=1, tiled=True),
        lax.all_gather(left_factor, "tp", axis=1, tiled=True),
        lax.all_gather(right_factor, "tp", axis=1, tiled=True),
    )
    depth = first_moment.shape[1]
    grad_query = lax.dot_general(left_proj, query_cotangent, TN, preferred_element_type=jnp.float32)
    grad_output = lax.dot_general(right_proj, attn_outputs, TN, preferred_element_type=jnp.float32)
    summed = lax.psum_scatter(
        jnp.stack([grad_query, grad_output], axis=1), "fs", scatter_dimension=0, tiled=True
    )
    grads = jnp.transpose(summed, (1, 0, 2))
    first_new, second_new, own_direction = moment_step(first_moment, second_moment, grads)
    direction_all = lax.all_gather(own_direction.astype(jnp.bfloat16), "fs", axis=1, tiled=True)
    squares = jnp.sum(own_direction * own_direction, axis=(1, 2))
    total = lax.psum(squares, ("fs", "tp"))
    entries = depth * lax.axis_size("fs") * own_direction.shape[2] * lax.axis_size("tp")
    scale = lax.rsqrt(total / entries + 1e-06)
    step_query = scale[0] * jnp.dot(left_rows, direction_all[0], preferred_element_type=jnp.float32)
    step_output = scale[1] * lax.dot_general(
        direction_all[1], right_rows, (((0,), (1,)), ((), ())), preferred_element_type=jnp.float32
    )
    query_new = query_master - 0.01 * step_query
    out_new = out_master - 0.01 * step_output
    query_copy, out_copy = (
        lax.all_gather(query_new.astype(jnp.bfloat16), "fs", axis=0, tiled=True),
        lax.all_gather(out_new.astype(jnp.bfloat16), "fs", axis=1, tiled=True),
    )
    return (query_new, out_new, query_copy, out_copy, first_new, second_new)


def choose_body(n_fs, n_tp, *args):
    left_factor, first_moment = args[4], args[8]
    model, part = args[0].shape[1], left_factor.shape[1]
    aligned = part % 16 == 0 and first_moment.shape[1] % 16 == 0
    aligned = aligned and model // n_fs % 128 == 0 and first_moment.shape[2] % 256 == 0
    aligned = aligned and first_moment.shape[2] % (model // n_fs) == 0
    if aligned and n_fs == PAIR * LINE and n_tp % PAIR == 0:
        return fast_body(n_fs, n_tp, *args)
    return plain_body(*args)


def solution(mesh):
    return jax.shard_map(
        functools.partial(choose_body, mesh.shape["fs"], mesh.shape["tp"]),
        mesh=mesh,
        in_specs=(
            P("fs", None),
            P("fs", "tp"),
            P("fs", "tp"),
            P("fs", None),
            P("fs", "tp"),
            P("fs", "tp"),
            P("fs", "tp"),
            P("tp", "fs"),
            P(None, "fs", "tp"),
            P(None, "fs", "tp"),
        ),
        out_specs=(
            P("fs", "tp"),
            P("tp", "fs"),
            P(None, "tp"),
            P("tp", None),
            P(None, "fs", "tp"),
            P(None, "fs", "tp"),
        ),
        check_vma=False,
    )
```

```python
import functools

import jax
import jax.numpy as jnp
from jax import lax
from jax.experimental import pallas as pl
from jax.experimental.pallas import tpu as pltpu
from jax.sharding import PartitionSpec as P

MESH = pl.DeviceIdType.MESH
PAIR = 2
LINE = 4
LANES = 128
EARLY_QUERY = 1
EARLY_OUT = 1
STORES = 4
FACTOR_CUTS = 1
DIRECTION_CUTS = 2
QUERY_ODD = (True, False, True)
OUT_ODD = (True, False, True)
NT = (((1,), (1,)), ((), ()))
TN = (((0,), (0,)), ((), ()))


def moment_step(first, second, grads):
    first_next = 0.9 * first + 0.1 * grads
    second_next = 0.99 * second + 0.01 * grads * grads
    return (first_next, second_next, first_next / (jnp.sqrt(second_next) + 1e-08))


def rows(index, size):
    return pl.ds(pl.multiple_of(index * size, size), size)


def peer_along(axis, index):
    if axis == "fs":
        return (index, lax.axis_index("tp"))
    return (lax.axis_index("fs"), index)


class Gather:
    def __init__(self, axis, count, view, sems, own=None):
        self.axis, self.outer, self.view, self.sems = axis, count // PAIR, view, sems
        me = lax.axis_index(axis)
        self.high, self.low = me // PAIR, lax.rem(me, PAIR)
        self.own = view(me) if own is None else own
        self.me = me

    def copy(self, src, dst, stage, slot, target):
        return pltpu.make_async_remote_copy(
            src_ref=src,
            dst_ref=dst,
            send_sem=self.sems.at[stage, 0, slot],
            recv_sem=self.sems.at[stage, 1, slot],
            device_id=peer_along(self.axis, target),
            device_id_type=MESH,
        )

    def index(self, offset, low):
        return lax.rem(self.high + offset, self.outer) * PAIR + low

    def outward(self, offset):
        return self.copy(self.own, self.view(self.me), 0, offset, self.index(offset, self.low))

    def inward(self, offset):
        source = self.index(self.outer - offset, self.low)
        src = self.own if offset == 0 else self.view(source)
        partner = self.high * PAIR + 1 - self.low
        return self.copy(src, self.view(self.me if offset == 0 else source), 1, offset, partner)

    def start_outward(self):
        for offset in range(self.outer - 1, 0, -1):
            self.outward(offset).start()

    def start_inward(self):
        self.inward(0).start()

    def start(self):
        self.start_outward()
        self.start_inward()

    def forward(self):
        for offset in range(self.outer - 1, 0, -1):
            self.outward(offset).wait_recv()
            self.inward(offset).start()

    def finish(self):
        for offset in range(self.outer):
            self.inward(offset).wait_recv()
        for offset in range(1, self.outer):
            self.outward(offset).wait_send()
        for offset in range(self.outer):
            self.inward(offset).wait_send()


class Place:
    def __init__(self, outer):
        me, self.column = lax.axis_index("fs"), lax.axis_index("tp")
        self.me, self.low, self.outer = me, lax.rem(me, PAIR), outer
        self.z = me // PAIR
        self.near = self.z + 1 - 2 * lax.rem(self.z, 2)
        self.cross = outer - 1 - self.z
        self.skew = outer - 1 - self.near
        self.end = jnp.logical_or(self.z == 0, self.z == outer - 1)
        self.inner = jnp.logical_not(self.end)

    def same(self, z):
        return z * PAIR + self.low

    def other(self, z):
        return z * PAIR + 1 - self.low


class Spread:
    def __init__(self, place, view, span, send_sem, recv_sems, odd, own=None):
        self.place, self.view, self.span, self.odd = place, view, span, odd
        self.send_sem, self.recv_sems = send_sem, recv_sems
        self.own = view(place.me) if own is None else own

    def remote(self, src, dst, recv, target):
        return pltpu.make_async_remote_copy(
            src_ref=src,
            dst_ref=dst,
            send_sem=self.send_sem,
            recv_sem=self.recv_sems.at[recv],
            device_id=(target, self.place.column),
            device_id_type=MESH,
        )

    def mine(self, recv, target):
        return self.remote(self.own, self.view(self.place.me), recv, target)

    def passed(self, block, recv, target):
        return self.remote(self.view(block), self.view(block), recv, target)

    def to_skew(self):
        return self.mine(0, self.place.same(self.place.skew))

    def to_near(self):
        return self.mine(1, self.place.same(self.place.near))

    def to_cross(self):
        return self.mine(2, self.place.same(self.place.cross))

    def to_pair(self):
        return self.mine(3, self.place.other(self.place.z))

    def pair_on(self, z):
        return self.passed(self.place.same(z), 4, self.place.other(self.place.z))

    def relay_skew(self):
        return self.passed(self.place.same(self.place.skew), 2, self.place.same(self.place.near))

    def relay_pair(self):
        return self.passed(self.place.other(self.place.z), 4, self.place.same(self.place.near))

    def launch(self):
        self.launch_pair()
        self.launch_skew()
        self.launch_near()
        self.launch_cross()

    def launch_pair(self):
        self.to_pair().start()

    def launch_skew(self):
        self.to_skew().start()

    def launch_near(self):
        self.to_near().start()

    def launch_cross(self):
        pl.when(self.place.inner)(lambda: self.to_cross().start())

    def hop(self):
        self.to_skew().wait_recv()
        pl.when(self.place.inner)(lambda: self.relay_skew().start())

    def pass_skew(self):
        self.pair_on(self.place.skew).start()

    def pass_near(self):
        if not self.odd:
            self.to_near().wait_recv()
            pl.when(self.place.end)(lambda: self.pair_on(self.place.near).start())

    def pass_pair(self):
        self.to_pair().wait_recv()
        if self.odd:
            self.relay_pair().start()
        else:
            pl.when(self.place.end)(lambda: self.relay_pair().start())

    def pass_cross(self):
        self.to_cross().wait_recv()
        self.pair_on(self.place.cross).start()

    def relay(self):
        self.hop()
        self.pass_skew()
        self.pass_near()

    def many(self, count):
        return self.remote(self.span(count), self.span(count), 4, self.place.other(self.place.z))

    def collect(self):
        if self.odd:
            self.to_near().wait_recv()
        self.many(3).wait_recv()

    def drain(self):
        if self.odd:
            pl.when(self.place.end)(lambda: self.many(6).wait_send())
            pl.when(self.place.inner)(lambda: self.many(8).wait_send())
        else:
            self.many(7).wait_send()


def kernel(
    n_fs,
    n_tp,
    early_query,
    early_out,
    saved_hbm,
    outcot_hbm,
    querycot_hbm,
    attn_hbm,
    query_hbm,
    out_hbm,
    left_hbm,
    right_hbm,
    first_hbm,
    second_hbm,
    query_out,
    out_out,
    query_copy,
    out_copy,
    first_out,
    second_out,
    factor_ref,
    first_ref,
    second_ref,
    factors_ref,
    own_rows,
    dirs_ref,
    query_master,
    out_master,
    query_early,
    out_early,
    saved,
    outcot,
    querycot,
    attn,
    proj,
    grad,
    pair_send,
    pair_recv,
    far_send,
    far_recv,
    own_dir,
    square_buf,
    load_sems,
    rows_sems,
    proj_sems,
    columns_sems,
    pair_sems,
    far_sems,
    wire_sems,
    square_sems,
    spread_sends,
    spread_recvs,
):
    outer = n_fs // PAIR
    place = Place(outer)
    me, column, high, low = place.me, place.column, place.z, place.low
    part = factor_ref.shape[1]
    width = factor_ref.shape[2]
    depth = first_ref.shape[1]
    features = grad.shape[2]
    pieces = width // LANES
    tall, deep = LANES, features // pieces
    loads = [
        pltpu.make_async_copy(src, dst, load_sems.at[i])
        for i, (src, dst) in enumerate(
            (
                (saved_hbm, saved),
                (outcot_hbm, outcot),
                (querycot_hbm, querycot),
                (attn_hbm, attn),
                (query_hbm, query_master),
                (out_hbm, out_master),
                (first_hbm, first_ref),
                (second_hbm, second_ref),
                (left_hbm, factor_ref.at[0]),
                (right_hbm, factor_ref.at[1]),
            )
        )
    ]

    fs_peers = [(lax.rem(me + i, n_fs), column) for i in range(1, n_fs)]
    tp_peers = [(me, lax.rem(column + i, n_tp)) for i in range(1, n_tp)]
    barrier = pltpu.get_barrier_semaphore()
    for peer in fs_peers + tp_peers:
        pl.semaphore_signal(barrier, inc=1, device_id=peer, device_id_type=MESH)
    for load in loads[8:] + loads[4:8] + loads[:4]:
        load.start()
    for load in loads[8:]:
        load.wait()
    pl.semaphore_wait(barrier, len(fs_peers) + len(tp_peers))

    def launch_all(gathers):
        for gather in gathers:
            gather.launch_pair()
        for gather in gathers:
            gather.launch_skew()
            if not gather.odd:
                gather.launch_near()
        for gather in gathers:
            gather.launch_cross()
            if gather.odd:
                gather.launch_near()

    def spread(slot, view, span, odd, own=None):
        return Spread(place, view, span, spread_sends.at[slot], spread_recvs.at[slot], odd, own)

    def factor_piece(k, c):
        band = part // FACTOR_CUTS
        start = pl.multiple_of(column * part + c * band, 16)
        return spread(
            k * FACTOR_CUTS + c,
            lambda i: factors_ref.at[k, pl.ds(start, band), rows(i, width)],
            lambda n: factors_ref.at[k, :band, : n * width],
            (k * FACTOR_CUTS + c) % 2 == 1,
            factor_ref.at[k, c * band : (c + 1) * band],
        )

    def direction_piece(k, c):
        band = features // DIRECTION_CUTS
        return spread(
            2 * FACTOR_CUTS + k * DIRECTION_CUTS + c,
            lambda i: dirs_ref.at[k, rows(i, depth), c * band : (c + 1) * band],
            lambda n: dirs_ref.at[k, : n * depth, :band],
            (k * DIRECTION_CUTS + c) % 2 == 1,
            own_dir.at[k, :, c * band : (c + 1) * band],
        )

    factors = [factor_piece(k, c) for k in range(2) for c in range(FACTOR_CUTS)]
    launch_all(factors)
    own_columns = Gather("tp", n_tp, lambda i: own_rows.at[:, rows(i, part), :], rows_sems, own=factor_ref)
    own_columns.start()
    factors_ref[:, rows(column, part), rows(me, width)] = factor_ref[...]
    own_rows[:, rows(column, part), :] = factor_ref[...]

    first_bulk = 2 * (FACTOR_CUTS + DIRECTION_CUTS)

    def query_piece(i, own=None):
        return spread(
            first_bulk + i,
            lambda j: query_copy.at[pl.ds(pl.multiple_of(j * width + i * tall, tall), tall), :],
            lambda n: query_copy.at[: n * tall, :],
            QUERY_ODD[i % 3],
            own,
        )

    def out_piece(i, own=None):
        return spread(
            first_bulk + pieces + i,
            lambda j: out_copy.at[i * deep : (i + 1) * deep, rows(j, width)],
            lambda n: out_copy.at[:deep, : n * width],
            OUT_ODD[i % 3],
            own,
        )

    early_q = [query_piece(i, query_early.at[i]) for i in range(early_query)]
    early_o = [out_piece(i, out_early.at[i]) for i in range(early_out)]
    late_q = [query_piece(i) for i in range(early_query, pieces)]
    late_o = [out_piece(i) for i in range(early_out, pieces)]

    loads[4].wait()
    for i in range(early_query):
        query_early[i] = query_master[i * tall : (i + 1) * tall, :].astype(query_early.dtype)
    loads[5].wait()
    for i in range(early_out):
        out_early[i] = out_master[i * deep : (i + 1) * deep, :].astype(out_early.dtype)
    for gather in factors:
        gather.relay()
    for gather in factors:
        gather.pass_pair()
    for gather in factors:
        gather.pass_cross()
    for gather in early_q:
        gather.launch_skew()
        gather.launch_near()
        gather.launch_cross()
    for gather in early_o:
        gather.launch_pair()
        gather.launch_near()
    own_columns.forward()

    def project(k, tokens, origins):
        total = None
        for origin in origins:
            product = lax.dot_general(
                factors_ref[k, rows(column, part), rows(origin, width)],
                tokens[:, rows(origin, width)],
                NT,
                preferred_element_type=jnp.float32,
            )
            total = product if total is None else total + product
        return total

    first_origins = (me, place.same(place.skew), place.same(place.cross), place.other(place.z))
    last_origins = (place.same(place.near),) + tuple(
        place.other(z) for z in (place.skew, place.near, place.cross)
    )
    first_proj = []
    for k, tokens in enumerate((saved, outcot)):
        loads[k].wait()
        first_proj.append(project(k, tokens, first_origins))
    gathers = []
    for k, tokens in enumerate((saved, outcot)):
        for gather in factors[k * FACTOR_CUTS : (k + 1) * FACTOR_CUTS]:
            gather.collect()
        part_proj = first_proj[k] + project(k, tokens, last_origins)
        proj[k, rows(column, part), :] = part_proj.astype(proj.dtype)
        gather = Gather(
            "tp", n_tp, lambda i, k=k: proj.at[k, rows(i, part), :], proj_sems.at[k]
        )
        gather.start()
        gathers.append(gather)

    blocks = (place.cross, place.skew, place.near, place.z)

    def pair_copy(r, k):
        return pltpu.make_async_remote_copy(
            src_ref=pair_send.at[r, k],
            dst_ref=pair_recv.at[r, k],
            send_sem=wire_sems.at[0],
            recv_sem=pair_sems.at[r, k],
            device_id=(place.other(place.z), column),
            device_id_type=MESH,
        )

    def far_copy(r, k, slot, z):
        return pltpu.make_async_remote_copy(
            src_ref=far_send.at[r, k],
            dst_ref=far_recv.at[slot, k],
            send_sem=wire_sems.at[1],
            recv_sem=far_sems.at[slot, k],
            device_id=(place.same(z), column),
            device_id_type=MESH,
        )

    def both(r, k):
        return grad[k, rows(place.same(blocks[r]), depth), :] + pair_recv[r, k].astype(jnp.float32)

    columns = Gather("tp", n_tp, lambda i: factors_ref.at[:, rows(i, part), :], columns_sems)
    for k, (gather, cot) in enumerate(zip(gathers, (querycot, attn))):
        gather.forward()
        if k == 1:
            columns.start()
        gather.finish()
        loads[2 + k].wait()
        grad[k, :, :] = jnp.dot(proj[k], cot[...], preferred_element_type=jnp.float32)
        for r in range(outer):
            pair_send[r, k] = grad[k, rows(place.other(blocks[r]), depth), :].astype(pair_send.dtype)
            pair_copy(r, k).start()
    totals = []
    for k in range(2):
        for r in range(outer - 1):
            pair_copy(r, k).wait_recv()
            far_send[r, k] = both(r, k).astype(far_send.dtype)
            if r == outer - 2:
                far_copy(r, k, 2, place.near).start()
            else:
                pl.when(place.end)(lambda r=r, k=k: far_copy(r, k, 1 - r, place.near).start())
        pair_copy(outer - 1, k).wait_recv()
        totals.append(both(outer - 1, k))

        def add_near(k=k):
            for r in range(outer - 2):
                far_copy(r, k, r, place.near).wait_recv()
                far_send[r, k] = (both(r, k) + far_recv[r, k].astype(jnp.float32)).astype(far_send.dtype)
                far_copy(r, k, 3, blocks[r]).start()

        pl.when(place.inner)(add_near)
        if k == 0:
            for gather in early_q:
                gather.hop()
    for gather in early_q:
        gather.pass_skew()
    for k in range(2):
        for slot in (2, 3):
            far_copy(0, k, slot, place.near).wait_recv()
            totals[k] = totals[k] + far_recv[slot, k].astype(jnp.float32)

    shape = square_buf.shape[1:]
    row = lax.broadcasted_iota(jnp.int32, shape, 0)
    mine = jnp.zeros(shape, jnp.float32)
    for load in loads[6:8]:
        load.wait()
    for k in range(2):
        first_new, second_new, direction = moment_step(first_ref[k], second_ref[k], totals[k])
        own_dir[k] = direction.astype(own_dir.dtype)
        first_out[k] = first_new
        second_out[k] = second_new
        mine = jnp.where(row == k, jnp.sum(direction * direction), mine)

    def square_copy(base, slot, stage, count, target):
        return pltpu.make_async_remote_copy(
            src_ref=square_buf.at[pl.ds(base, count)],
            dst_ref=square_buf.at[pl.ds(slot, count)],
            send_sem=square_sems.at[stage, 0],
            recv_sem=square_sems.at[stage, 1],
            device_id=target,
            device_id_type=MESH,
        )

    def square_all(base, count, stage):
        return square_copy(base, base + 1, stage, count, tp_peers[0])

    square_buf[0] = mine
    for i, peer in enumerate(fs_peers):
        square_copy(0, 1 + i, 0, 1, peer).start()
    dirs = [direction_piece(k, c) for k in range(2) for c in range(DIRECTION_CUTS)]
    launch_all(dirs)
    for gather in early_q:
        gather.launch_pair()
    dirs_ref[:, rows(me, depth), :] = own_dir[...]
    for gather in dirs:
        gather.relay()
    for gather in dirs:
        gather.pass_pair()
    for gather in early_q:
        gather.pass_near()
        gather.pass_pair()
    for gather in early_o:
        gather.pass_pair()
    for gather in early_o:
        gather.launch_skew()
        gather.launch_cross()
    square_all(0, n_fs - 1, 0).wait_recv()
    mine = jnp.sum(square_buf[:n_fs], axis=0)
    square_buf[n_fs] = mine
    for i, peer in enumerate(tp_peers):
        square_copy(n_fs, n_fs + 1 + i, 1, 1, peer).start()
    for gather in dirs:
        gather.pass_cross()
    square_all(n_fs, n_tp - 1, 1).wait_recv()
    mine = jnp.sum(square_buf[n_fs:], axis=0)
    entries = dirs_ref.shape[1] * dirs_ref.shape[2] * n_tp
    scale = 0.01 * lax.rsqrt(mine / entries + 1e-06)
    scales = (scale[0:1, 0:1], scale[1:2, 0:1])
    own_columns.finish()
    for gather in dirs:
        gather.collect()

    def launch_late(gathers):
        for gather in gathers:
            gather.launch_pair()
            gather.launch_skew()
            if not gather.odd:
                gather.launch_near()

    query_new = query_master[...] - scales[0] * lax.dot_general(
        own_rows[0], dirs_ref[0], TN, preferred_element_type=jnp.float32
    )
    query_out[...] = query_new
    query_copy[rows(me, width), :] = query_new.astype(query_copy.dtype)
    launch_late(late_q)
    out_new = out_master[...] - scales[1] * lax.dot_general(
        dirs_ref[1], own_rows[1], TN, preferred_element_type=jnp.float32
    )
    out_out[...] = out_new
    out_copy[:, rows(me, width)] = out_new.astype(out_copy.dtype)
    launch_late(late_o)
    for gather in late_q + late_o:
        gather.launch_cross()

    columns.forward()
    bulk = early_o + late_q + late_o

    def finish_near(gather):
        if gather not in early_o:
            if gather.odd:
                gather.launch_near()
            gather.pass_pair()

    crossing = early_q + bulk
    for i, gather in enumerate(bulk):
        gather.relay()
        if i >= 1:
            pl.when(place.end)(crossing[i + 1 - 2].pass_cross)
        if i >= 9:
            finish_near(bulk[i - 9])
    for gather in bulk[max(len(bulk) - 9, 0) :]:
        finish_near(gather)
    for gather in crossing[:-2]:
        pl.when(place.inner)(gather.pass_cross)
    for gather in crossing[-2:]:
        gather.pass_cross()
    columns.finish()

    for gather in early_q + early_o:
        gather.collect()
        gather.drain()

    def finish_block(i, carry):
        block = lax.rem(me + i, n_fs)
        for j in range(early_query):
            where = pl.ds(pl.multiple_of(block * width + j * tall, tall), tall)
            step = lax.dot_general(
                factors_ref[0, :, where], dirs_ref[0], TN, preferred_element_type=jnp.float32
            )
            query = query_copy[where, :].astype(jnp.float32)
            query_copy[where, :] = (query - scales[0] * step).astype(query_copy.dtype)
        for j in range(early_out):
            band = slice(j * deep, (j + 1) * deep)
            step = lax.dot_general(
                dirs_ref[1, :, band],
                factors_ref[1, :, rows(block, width)],
                TN,
                preferred_element_type=jnp.float32,
            )
            out = out_copy[band, rows(block, width)].astype(jnp.float32)
            out_copy[band, rows(block, width)] = (out - scales[1] * step).astype(out_copy.dtype)
        return carry

    lax.fori_loop(1, n_fs, finish_block, 0)
    for gather in late_q + late_o:
        gather.collect()
    for gather in factors + dirs + late_q + late_o:
        gather.drain()
    pltpu.make_async_copy(pair_send, pair_recv, wire_sems.at[0]).wait()
    pltpu.make_async_copy(far_send.at[1:], far_send.at[1:], wire_sems.at[1]).wait()
    square_all(0, n_fs - 1, 0).wait_send()
    square_all(n_fs, n_tp - 1, 1).wait_send()


def store_kernel(*refs):
    count = len(refs) // 2
    sems = refs[-1]
    copies = []
    for i in range(count):
        size = refs[i].shape[0] // STORES if refs[i].shape[0] % (16 * STORES) == 0 else refs[i].shape[0]
        for j in range(refs[i].shape[0] // size):
            band = slice(j * size, (j + 1) * size)
            copies.append(pltpu.make_async_copy(refs[i].at[band], refs[count + i].at[band], sems.at[i, j]))
    for copy in copies:
        copy.start()
    for copy in copies:
        copy.wait()


def fast_body(
    n_fs,
    n_tp,
    saved_inputs,
    query_cotangent,
    attn_outputs,
    out_cotangent,
    left_factor,
    right_factor,
    query_master,
    out_master,
    first_moment,
    second_moment,
):
    tokens, model = saved_inputs.shape
    features = query_cotangent.shape[1]
    width, part = left_factor.shape
    depth = first_moment.shape[1]
    rank = part * n_tp
    outer = n_fs // PAIR
    pieces = width // LANES
    slots = 2 * (FACTOR_CUTS + DIRECTION_CUTS + pieces)
    low, wide = jnp.bfloat16, jnp.float32
    vmem = pl.BlockSpec(memory_space=pltpu.VMEM)
    anywhere = pl.BlockSpec(memory_space=pl.ANY)
    dma = pltpu.SemaphoreType.DMA
    results = pl.pallas_call(
        functools.partial(kernel, n_fs, n_tp, EARLY_QUERY, EARLY_OUT),
        out_shape=(
            pltpu.VMEM((width, features), wide),
            pltpu.VMEM((features, width), wide),
            pltpu.VMEM((model, features), low),
            pltpu.VMEM((features, model), low),
            pltpu.VMEM(first_moment.shape, wide),
            pltpu.VMEM(first_moment.shape, wide),
        ),
        in_specs=[anywhere] * 10,
        out_specs=(vmem,) * 6,
        scratch_shapes=[
            pltpu.VMEM((2, part, width), low),
            pltpu.VMEM(first_moment.shape, wide),
            pltpu.VMEM(first_moment.shape, wide),
            pltpu.VMEM((2, rank, model), low),
            pltpu.VMEM((2, rank, width), low),
            pltpu.VMEM((2, rank, features), low),
            pltpu.VMEM((width, features), wide),
            pltpu.VMEM((features, width), wide),
            pltpu.VMEM((max(EARLY_QUERY, 1), LANES, features), low),
            pltpu.VMEM((max(EARLY_OUT, 1), features // pieces, width), low),
            pltpu.VMEM((tokens, model), low),
            pltpu.VMEM((tokens, model), low),
            pltpu.VMEM((tokens, features), low),
            pltpu.VMEM((tokens, features), low),
            pltpu.VMEM((2, rank, tokens), low),
            pltpu.VMEM((2, rank, features), wide),
            pltpu.VMEM((outer, 2, depth, features), low),
            pltpu.VMEM((outer, 2, depth, features), low),
            pltpu.VMEM((outer, 2, depth, features), low),
            pltpu.VMEM((outer, 2, depth, features), low),
            pltpu.VMEM((2, depth, features), low),
            pltpu.VMEM((n_fs + n_tp, 8, 128), wide),
            dma((10,)),
            dma((2, 2, n_tp // PAIR)),
            dma((2, 2, 2, n_tp // PAIR)),
            dma((2, 2, n_tp // PAIR)),
            dma((outer, 2)),
            dma((outer, 2)),
            dma((2,)),
            dma((2, 2)),
            dma((slots,)),
            dma((slots, 5)),
        ],
        compiler_params=pltpu.CompilerParams(
            collective_id=0, has_side_effects=True, vmem_limit_bytes=46 * 2**20
        ),
        cost_estimate=pl.CostEstimate(
            flops=4 * tokens * rank * (model + features), bytes_accessed=200 * 2**20, transcendentals=0
        ),
    )(
        saved_inputs,
        out_cotangent,
        query_cotangent,
        attn_outputs,
        query_master,
        out_master,
        left_factor.T,
        right_factor.T,
        first_moment,
        second_moment,
    )
    return pl.pallas_call(
        store_kernel,
        out_shape=tuple(jax.ShapeDtypeStruct(r.shape, r.dtype) for r in results),
        in_specs=[vmem] * len(results),
        out_specs=(anywhere,) * len(results),
        scratch_shapes=[dma((len(results), STORES))],
        compiler_params=pltpu.CompilerParams(vmem_limit_bytes=2**20),
        cost_estimate=pl.CostEstimate(flops=2**20, bytes_accessed=13 * 2**20, transcendentals=0),
    )(*(pltpu.with_memory_space_constraint(r, pltpu.VMEM) for r in results))


def plain_body(
    saved_inputs,
    query_cotangent,
    attn_outputs,
    out_cotangent,
    left_factor,
    right_factor,
    query_master,
    out_master,
    first_moment,
    second_moment,
):
    left_part = jnp.dot(
        saved_inputs,
        lax.all_gather(left_factor, "fs", axis=0, tiled=True),
        preferred_element_type=jnp.float32,
    )
    right_part = jnp.dot(
        out_cotangent,
        lax.all_gather(right_factor, "fs", axis=0, tiled=True),
        preferred_element_type=jnp.float32,
    )
    left_proj, right_proj, left_rows, right_rows = (
        lax.all_gather(left_part.astype(jnp.bfloat16), "tp", axis=1, tiled=True),
        lax.all_gather(right_part.astype(jnp.bfloat16), "tp", axis=1, tiled=True),
        lax.all_gather(left_factor, "tp", axis=1, tiled=True),
        lax.all_gather(right_factor, "tp", axis=1, tiled=True),
    )
    depth = first_moment.shape[1]
    grad_query = lax.dot_general(left_proj, query_cotangent, TN, preferred_element_type=jnp.float32)
    grad_output = lax.dot_general(right_proj, attn_outputs, TN, preferred_element_type=jnp.float32)
    summed = lax.psum_scatter(
        jnp.stack([grad_query, grad_output], axis=1), "fs", scatter_dimension=0, tiled=True
    )
    grads = jnp.transpose(summed, (1, 0, 2))
    first_new, second_new, own_direction = moment_step(first_moment, second_moment, grads)
    direction_all = lax.all_gather(own_direction.astype(jnp.bfloat16), "fs", axis=1, tiled=True)
    squares = jnp.sum(own_direction * own_direction, axis=(1, 2))
    total = lax.psum(squares, ("fs", "tp"))
    entries = depth * lax.axis_size("fs") * own_direction.shape[2] * lax.axis_size("tp")
    scale = lax.rsqrt(total / entries + 1e-06)
    step_query = scale[0] * jnp.dot(left_rows, direction_all[0], preferred_element_type=jnp.float32)
    step_output = scale[1] * lax.dot_general(
        direction_all[1], right_rows, (((0,), (1,)), ((), ())), preferred_element_type=jnp.float32
    )
    query_new = query_master - 0.01 * step_query
    out_new = out_master - 0.01 * step_output
    query_copy, out_copy = (
        lax.all_gather(query_new.astype(jnp.bfloat16), "fs", axis=0, tiled=True),
        lax.all_gather(out_new.astype(jnp.bfloat16), "fs", axis=1, tiled=True),
    )
    return (query_new, out_new, query_copy, out_copy, first_new, second_new)


def choose_body(n_fs, n_tp, *args):
    left_factor, first_moment = args[4], args[8]
    model, part = args[0].shape[1], left_factor.shape[1]
    aligned = part % (16 * FACTOR_CUTS) == 0 and first_moment.shape[1] % 16 == 0
    aligned = aligned and model // n_fs % 128 == 0 and first_moment.shape[2] % (128 * DIRECTION_CUTS) == 0
    aligned = aligned and first_moment.shape[2] % (model // n_fs) == 0
    if aligned and n_fs == PAIR * LINE and n_tp % PAIR == 0:
        return fast_body(n_fs, n_tp, *args)
    return plain_body(*args)


def solution(mesh):
    return jax.shard_map(
        functools.partial(choose_body, mesh.shape["fs"], mesh.shape["tp"]),
        mesh=mesh,
        in_specs=(
            P("fs", None),
            P("fs", "tp"),
            P("fs", "tp"),
            P("fs", None),
            P("fs", "tp"),
            P("fs", "tp"),
            P("fs", "tp"),
            P("tp", "fs"),
            P(None, "fs", "tp"),
            P(None, "fs", "tp"),
        ),
        out_specs=(
            P("fs", "tp"),
            P("tp", "fs"),
            P(None, "tp"),
            P("tp", None),
            P(None, "fs", "tp"),
            P(None, "fs", "tp"),
        ),
        check_vma=False,
    )
```

```python
import functools

import jax
import jax.numpy as jnp
from jax import lax
from jax.experimental import pallas as pl
from jax.experimental.pallas import tpu as pltpu
from jax.sharding import PartitionSpec as P

MESH = pl.DeviceIdType.MESH
PAIR = 2
LINE = 4
LANES = 128
EARLY_QUERY = 1
EARLY_OUT = 1
STORES = 1
FACTOR_CUTS = 1
DIRECTION_CUTS = 2
QUERY_ODD = (True, False, True)
OUT_ODD = (True, False, True)
NT = (((1,), (1,)), ((), ()))
TN = (((0,), (0,)), ((), ()))


def moment_step(first, second, grads):
    first_next = 0.9 * first + 0.1 * grads
    second_next = 0.99 * second + 0.01 * grads * grads
    return (first_next, second_next, first_next / (jnp.sqrt(second_next) + 1e-08))


def rows(index, size):
    return pl.ds(pl.multiple_of(index * size, size), size)


def peer_along(axis, index):
    if axis == "fs":
        return (index, lax.axis_index("tp"))
    return (lax.axis_index("fs"), index)


class Gather:
    def __init__(self, axis, count, view, sems, own=None):
        self.axis, self.outer, self.view, self.sems = axis, count // PAIR, view, sems
        me = lax.axis_index(axis)
        self.high, self.low = me // PAIR, lax.rem(me, PAIR)
        self.own = view(me) if own is None else own
        self.me = me

    def copy(self, src, dst, stage, slot, target):
        return pltpu.make_async_remote_copy(
            src_ref=src,
            dst_ref=dst,
            send_sem=self.sems.at[stage, 0, slot],
            recv_sem=self.sems.at[stage, 1, slot],
            device_id=peer_along(self.axis, target),
            device_id_type=MESH,
        )

    def index(self, offset, low):
        return lax.rem(self.high + offset, self.outer) * PAIR + low

    def outward(self, offset):
        return self.copy(self.own, self.view(self.me), 0, offset, self.index(offset, self.low))

    def inward(self, offset):
        source = self.index(self.outer - offset, self.low)
        src = self.own if offset == 0 else self.view(source)
        partner = self.high * PAIR + 1 - self.low
        return self.copy(src, self.view(self.me if offset == 0 else source), 1, offset, partner)

    def start_outward(self):
        for offset in range(self.outer - 1, 0, -1):
            self.outward(offset).start()

    def start_inward(self):
        self.inward(0).start()

    def start(self):
        self.start_outward()
        self.start_inward()

    def forward(self):
        for offset in range(self.outer - 1, 0, -1):
            self.outward(offset).wait_recv()
            self.inward(offset).start()

    def finish(self):
        for offset in range(self.outer):
            self.inward(offset).wait_recv()
        for offset in range(1, self.outer):
            self.outward(offset).wait_send()
        for offset in range(self.outer):
            self.inward(offset).wait_send()


class Place:
    def __init__(self, outer):
        me, self.column = lax.axis_index("fs"), lax.axis_index("tp")
        self.me, self.low, self.outer = me, lax.rem(me, PAIR), outer
        self.z = me // PAIR
        self.near = self.z + 1 - 2 * lax.rem(self.z, 2)
        self.cross = outer - 1 - self.z
        self.skew = outer - 1 - self.near
        self.end = jnp.logical_or(self.z == 0, self.z == outer - 1)
        self.inner = jnp.logical_not(self.end)

    def same(self, z):
        return z * PAIR + self.low

    def other(self, z):
        return z * PAIR + 1 - self.low


class Spread:
    def __init__(self, place, view, span, send_sem, recv_sems, odd, own=None):
        self.place, self.view, self.span, self.odd = place, view, span, odd
        self.send_sem, self.recv_sems = send_sem, recv_sems
        self.own = view(place.me) if own is None else own

    def remote(self, src, dst, recv, target):
        return pltpu.make_async_remote_copy(
            src_ref=src,
            dst_ref=dst,
            send_sem=self.send_sem,
            recv_sem=self.recv_sems.at[recv],
            device_id=(target, self.place.column),
            device_id_type=MESH,
        )

    def mine(self, recv, target):
        return self.remote(self.own, self.view(self.place.me), recv, target)

    def passed(self, block, recv, target):
        return self.remote(self.view(block), self.view(block), recv, target)

    def to_skew(self):
        return self.mine(0, self.place.same(self.place.skew))

    def to_near(self):
        return self.mine(1, self.place.same(self.place.near))

    def to_cross(self):
        return self.mine(2, self.place.same(self.place.cross))

    def to_pair(self):
        return self.mine(3, self.place.other(self.place.z))

    def pair_on(self, z):
        return self.passed(self.place.same(z), 4, self.place.other(self.place.z))

    def relay_skew(self):
        return self.passed(self.place.same(self.place.skew), 2, self.place.same(self.place.near))

    def relay_pair(self):
        return self.passed(self.place.other(self.place.z), 4, self.place.same(self.place.near))

    def launch(self):
        self.launch_pair()
        self.launch_skew()
        self.launch_near()
        self.launch_cross()

    def launch_pair(self):
        self.to_pair().start()

    def launch_skew(self):
        self.to_skew().start()

    def launch_near(self):
        self.to_near().start()

    def launch_cross(self):
        pl.when(self.place.inner)(lambda: self.to_cross().start())

    def hop(self):
        self.to_skew().wait_recv()
        pl.when(self.place.inner)(lambda: self.relay_skew().start())

    def pass_skew(self):
        self.pair_on(self.place.skew).start()

    def pass_near(self):
        if not self.odd:
            self.to_near().wait_recv()
            pl.when(self.place.end)(lambda: self.pair_on(self.place.near).start())

    def pass_pair(self):
        self.to_pair().wait_recv()
        if self.odd:
            self.relay_pair().start()
        else:
            pl.when(self.place.end)(lambda: self.relay_pair().start())

    def pass_cross(self):
        self.to_cross().wait_recv()
        self.pair_on(self.place.cross).start()

    def relay(self):
        self.hop()
        self.pass_skew()
        self.pass_near()

    def many(self, count):
        return self.remote(self.span(count), self.span(count), 4, self.place.other(self.place.z))

    def collect(self):
        if self.odd:
            self.to_near().wait_recv()
        self.many(3).wait_recv()

    def drain(self):
        if self.odd:
            pl.when(self.place.end)(lambda: self.many(6).wait_send())
            pl.when(self.place.inner)(lambda: self.many(8).wait_send())
        else:
            self.many(7).wait_send()


def kernel(
    n_fs,
    n_tp,
    early_query,
    early_out,
    saved_hbm,
    outcot_hbm,
    querycot_hbm,
    attn_hbm,
    query_hbm,
    out_hbm,
    left_hbm,
    right_hbm,
    first_hbm,
    second_hbm,
    query_out,
    out_out,
    query_copy,
    out_copy,
    first_out,
    second_out,
    factor_ref,
    first_ref,
    second_ref,
    factors_ref,
    own_rows,
    dirs_ref,
    query_master,
    out_master,
    query_early,
    out_early,
    saved,
    outcot,
    querycot,
    attn,
    proj,
    grad,
    pair_send,
    pair_recv,
    far_send,
    far_recv,
    own_dir,
    square_buf,
    load_sems,
    rows_sems,
    proj_sems,
    columns_sems,
    pair_sems,
    far_sems,
    wire_sems,
    square_sems,
    spread_sends,
    spread_recvs,
):
    outer = n_fs // PAIR
    place = Place(outer)
    me, column, high, low = place.me, place.column, place.z, place.low
    part = factor_ref.shape[1]
    width = factor_ref.shape[2]
    depth = first_ref.shape[1]
    features = grad.shape[2]
    pieces = width // LANES
    tall, deep = LANES, features // pieces
    loads = [
        pltpu.make_async_copy(src, dst, load_sems.at[i])
        for i, (src, dst) in enumerate(
            (
                (saved_hbm, saved),
                (outcot_hbm, outcot),
                (querycot_hbm, querycot),
                (attn_hbm, attn),
                (query_hbm, query_master),
                (out_hbm, out_master),
                (first_hbm, first_ref),
                (second_hbm, second_ref),
                (left_hbm, factor_ref.at[0]),
                (right_hbm, factor_ref.at[1]),
            )
        )
    ]

    fs_peers = [(lax.rem(me + i, n_fs), column) for i in range(1, n_fs)]
    tp_peers = [(me, lax.rem(column + i, n_tp)) for i in range(1, n_tp)]
    barrier = pltpu.get_barrier_semaphore()
    for peer in fs_peers + tp_peers:
        pl.semaphore_signal(barrier, inc=1, device_id=peer, device_id_type=MESH)
    for load in loads[8:] + loads[4:8] + loads[:4]:
        load.start()
    for load in loads[8:]:
        load.wait()
    pl.semaphore_wait(barrier, len(fs_peers) + len(tp_peers))

    def launch_all(gathers):
        for gather in gathers:
            gather.launch_pair()
        for gather in gathers:
            gather.launch_skew()
            if not gather.odd:
                gather.launch_near()
        for gather in gathers:
            gather.launch_cross()
            if gather.odd:
                gather.launch_near()

    def spread(slot, view, span, odd, own=None):
        return Spread(place, view, span, spread_sends.at[slot], spread_recvs.at[slot], odd, own)

    def factor_piece(k, c):
        band = part // FACTOR_CUTS
        start = pl.multiple_of(column * part + c * band, 16)
        return spread(
            k * FACTOR_CUTS + c,
            lambda i: factors_ref.at[k, pl.ds(start, band), rows(i, width)],
            lambda n: factors_ref.at[k, :band, : n * width],
            (k * FACTOR_CUTS + c) % 2 == 1,
            factor_ref.at[k, c * band : (c + 1) * band],
        )

    def direction_piece(k, c):
        band = features // DIRECTION_CUTS
        return spread(
            2 * FACTOR_CUTS + k * DIRECTION_CUTS + c,
            lambda i: dirs_ref.at[k, rows(i, depth), c * band : (c + 1) * band],
            lambda n: dirs_ref.at[k, : n * depth, :band],
            (k * DIRECTION_CUTS + c) % 2 == 1,
            own_dir.at[k, :, c * band : (c + 1) * band],
        )

    factors = [factor_piece(k, c) for k in range(2) for c in range(FACTOR_CUTS)]
    launch_all(factors)
    own_columns = Gather("tp", n_tp, lambda i: own_rows.at[:, rows(i, part), :], rows_sems, own=factor_ref)
    own_columns.start()
    factors_ref[:, rows(column, part), rows(me, width)] = factor_ref[...]
    own_rows[:, rows(column, part), :] = factor_ref[...]

    first_bulk = 2 * (FACTOR_CUTS + DIRECTION_CUTS)

    def query_piece(i, own=None):
        return spread(
            first_bulk + i,
            lambda j: query_copy.at[pl.ds(pl.multiple_of(j * width + i * tall, tall), tall), :],
            lambda n: query_copy.at[: n * tall, :],
            QUERY_ODD[i % 3],
            own,
        )

    def out_piece(i, own=None):
        return spread(
            first_bulk + pieces + i,
            lambda j: out_copy.at[i * deep : (i + 1) * deep, rows(j, width)],
            lambda n: out_copy.at[:deep, : n * width],
            OUT_ODD[i % 3],
            own,
        )

    early_q = [query_piece(i, query_early.at[i]) for i in range(early_query)]
    early_o = [out_piece(i, out_early.at[i]) for i in range(early_out)]
    late_q = [query_piece(i) for i in range(early_query, pieces)]
    late_o = [out_piece(i) for i in range(early_out, pieces)]

    loads[4].wait()
    for i in range(early_query):
        query_early[i] = query_master[i * tall : (i + 1) * tall, :].astype(query_early.dtype)
    loads[5].wait()
    for i in range(early_out):
        out_early[i] = out_master[i * deep : (i + 1) * deep, :].astype(out_early.dtype)
    for gather in factors:
        gather.relay()
    for gather in factors:
        gather.pass_pair()
    for gather in factors:
        gather.pass_cross()
    for gather in early_q:
        gather.launch_skew()
        gather.launch_near()
        gather.launch_cross()
    for gather in early_o:
        gather.launch_pair()
        gather.launch_near()
    own_columns.forward()

    def project(k, tokens, origins):
        total = None
        for origin in origins:
            product = lax.dot_general(
                factors_ref[k, rows(column, part), rows(origin, width)],
                tokens[:, rows(origin, width)],
                NT,
                preferred_element_type=jnp.float32,
            )
            total = product if total is None else total + product
        return total

    first_origins = (me, place.same(place.skew), place.same(place.cross), place.other(place.z))
    last_origins = (place.same(place.near),) + tuple(
        place.other(z) for z in (place.skew, place.near, place.cross)
    )
    first_proj = []
    for k, tokens in enumerate((saved, outcot)):
        loads[k].wait()
        first_proj.append(project(k, tokens, first_origins))
    gathers = []
    for k, tokens in enumerate((saved, outcot)):
        for gather in factors[k * FACTOR_CUTS : (k + 1) * FACTOR_CUTS]:
            gather.collect()
        part_proj = first_proj[k] + project(k, tokens, last_origins)
        proj[k, rows(column, part), :] = part_proj.astype(proj.dtype)
        gather = Gather(
            "tp", n_tp, lambda i, k=k: proj.at[k, rows(i, part), :], proj_sems.at[k]
        )
        gather.start()
        gathers.append(gather)

    blocks = (place.cross, place.skew, place.near, place.z)

    def pair_copy(r, k):
        return pltpu.make_async_remote_copy(
            src_ref=pair_send.at[r, k],
            dst_ref=pair_recv.at[r, k],
            send_sem=wire_sems.at[0],
            recv_sem=pair_sems.at[r, k],
            device_id=(place.other(place.z), column),
            device_id_type=MESH,
        )

    def far_copy(r, k, slot, z):
        return pltpu.make_async_remote_copy(
            src_ref=far_send.at[r, k],
            dst_ref=far_recv.at[slot, k],
            send_sem=wire_sems.at[1],
            recv_sem=far_sems.at[slot, k],
            device_id=(place.same(z), column),
            device_id_type=MESH,
        )

    def both(r, k):
        return grad[k, rows(place.same(blocks[r]), depth), :] + pair_recv[r, k].astype(jnp.float32)

    columns = Gather("tp", n_tp, lambda i: factors_ref.at[:, rows(i, part), :], columns_sems)
    for k, (gather, cot) in enumerate(zip(gathers, (querycot, attn))):
        gather.forward()
        if k == 1:
            columns.start()
        gather.finish()
        loads[2 + k].wait()
        grad[k, :, :] = jnp.dot(proj[k], cot[...], preferred_element_type=jnp.float32)
        for r in range(outer):
            pair_send[r, k] = grad[k, rows(place.other(blocks[r]), depth), :].astype(pair_send.dtype)
            pair_copy(r, k).start()
    totals = []
    for k in range(2):
        for r in range(outer - 1):
            pair_copy(r, k).wait_recv()
            far_send[r, k] = both(r, k).astype(far_send.dtype)
            if r == outer - 2:
                far_copy(r, k, 2, place.near).start()
            else:
                pl.when(place.end)(lambda r=r, k=k: far_copy(r, k, 1 - r, place.near).start())
        pair_copy(outer - 1, k).wait_recv()
        totals.append(both(outer - 1, k))

        def add_near(k=k):
            for r in range(outer - 2):
                far_copy(r, k, r, place.near).wait_recv()
                far_send[r, k] = (both(r, k) + far_recv[r, k].astype(jnp.float32)).astype(far_send.dtype)
                far_copy(r, k, 3, blocks[r]).start()

        pl.when(place.inner)(add_near)
        if k == 0:
            for gather in early_q:
                gather.hop()
    for gather in early_q:
        gather.pass_skew()
    for k in range(2):
        for slot in (2, 3):
            far_copy(0, k, slot, place.near).wait_recv()
            totals[k] = totals[k] + far_recv[slot, k].astype(jnp.float32)

    shape = square_buf.shape[1:]
    row = lax.broadcasted_iota(jnp.int32, shape, 0)
    mine = jnp.zeros(shape, jnp.float32)
    for load in loads[6:8]:
        load.wait()
    for k in range(2):
        first_new, second_new, direction = moment_step(first_ref[k], second_ref[k], totals[k])
        own_dir[k] = direction.astype(own_dir.dtype)
        first_out[k] = first_new
        second_out[k] = second_new
        mine = jnp.where(row == k, jnp.sum(direction * direction), mine)

    def square_copy(base, slot, stage, count, target):
        return pltpu.make_async_remote_copy(
            src_ref=square_buf.at[pl.ds(base, count)],
            dst_ref=square_buf.at[pl.ds(slot, count)],
            send_sem=square_sems.at[stage, 0],
            recv_sem=square_sems.at[stage, 1],
            device_id=target,
            device_id_type=MESH,
        )

    def square_all(base, count, stage):
        return square_copy(base, base + 1, stage, count, tp_peers[0])

    square_buf[0] = mine
    for i, peer in enumerate(fs_peers):
        square_copy(0, 1 + i, 0, 1, peer).start()
    dirs = [direction_piece(k, c) for k in range(2) for c in range(DIRECTION_CUTS)]
    launch_all(dirs)
    for gather in early_q:
        gather.launch_pair()
    dirs_ref[:, rows(me, depth), :] = own_dir[...]
    for gather in dirs:
        gather.relay()
    for gather in dirs:
        gather.pass_pair()
    for gather in early_q:
        gather.pass_near()
        gather.pass_pair()
    for gather in early_o:
        gather.pass_pair()
    for gather in early_o:
        gather.launch_skew()
        gather.launch_cross()
    square_all(0, n_fs - 1, 0).wait_recv()
    mine = jnp.sum(square_buf[:n_fs], axis=0)
    square_buf[n_fs] = mine
    for i, peer in enumerate(tp_peers):
        square_copy(n_fs, n_fs + 1 + i, 1, 1, peer).start()
    for gather in dirs:
        gather.pass_cross()
    square_all(n_fs, n_tp - 1, 1).wait_recv()
    mine = jnp.sum(square_buf[n_fs:], axis=0)
    entries = dirs_ref.shape[1] * dirs_ref.shape[2] * n_tp
    scale = 0.01 * lax.rsqrt(mine / entries + 1e-06)
    scales = (scale[0:1, 0:1], scale[1:2, 0:1])
    own_columns.finish()
    for gather in dirs:
        gather.collect()

    def launch_late(gathers):
        for gather in gathers:
            gather.launch_pair()
            gather.launch_skew()
            if not gather.odd:
                gather.launch_near()

    query_new = query_master[...] - scales[0] * lax.dot_general(
        own_rows[0], dirs_ref[0], TN, preferred_element_type=jnp.float32
    )
    query_out[...] = query_new
    query_copy[rows(me, width), :] = query_new.astype(query_copy.dtype)
    launch_late(late_q)
    out_new = out_master[...] - scales[1] * lax.dot_general(
        dirs_ref[1], own_rows[1], TN, preferred_element_type=jnp.float32
    )
    out_out[...] = out_new
    out_copy[:, rows(me, width)] = out_new.astype(out_copy.dtype)
    launch_late(late_o)
    for gather in late_q + late_o:
        gather.launch_cross()

    columns.forward()
    bulk = early_o + late_q + late_o

    def finish_near(gather):
        if gather not in early_o:
            if gather.odd:
                gather.launch_near()
            gather.pass_pair()

    crossing = early_q + bulk
    for i, gather in enumerate(bulk):
        gather.relay()
        if i >= 1:
            pl.when(place.end)(crossing[i + 1 - 2].pass_cross)
        if i >= 9:
            finish_near(bulk[i - 9])
    for gather in bulk[max(len(bulk) - 9, 0) :]:
        finish_near(gather)
    for gather in crossing[:-2]:
        pl.when(place.inner)(gather.pass_cross)
    for gather in crossing[-2:]:
        gather.pass_cross()
    columns.finish()

    for gather in early_q + early_o:
        gather.collect()
        gather.drain()

    def finish_block(i, carry):
        block = lax.rem(me + i, n_fs)
        for j in range(early_query):
            where = pl.ds(pl.multiple_of(block * width + j * tall, tall), tall)
            step = lax.dot_general(
                factors_ref[0, :, where], dirs_ref[0], TN, preferred_element_type=jnp.float32
            )
            query = query_copy[where, :].astype(jnp.float32)
            query_copy[where, :] = (query - scales[0] * step).astype(query_copy.dtype)
        for j in range(early_out):
            band = slice(j * deep, (j + 1) * deep)
            step = lax.dot_general(
                dirs_ref[1, :, band],
                factors_ref[1, :, rows(block, width)],
                TN,
                preferred_element_type=jnp.float32,
            )
            out = out_copy[band, rows(block, width)].astype(jnp.float32)
            out_copy[band, rows(block, width)] = (out - scales[1] * step).astype(out_copy.dtype)
        return carry

    lax.fori_loop(1, n_fs, finish_block, 0)
    for gather in late_q + late_o:
        gather.collect()
    for gather in factors + dirs + late_q + late_o:
        gather.drain()
    pltpu.make_async_copy(pair_send, pair_recv, wire_sems.at[0]).wait()
    pltpu.make_async_copy(far_send.at[1:], far_send.at[1:], wire_sems.at[1]).wait()
    square_all(0, n_fs - 1, 0).wait_send()
    square_all(n_fs, n_tp - 1, 1).wait_send()


def store_kernel(*refs):
    count = len(refs) // 2
    sems = refs[-1]
    copies = []
    for i in range(count):
        size = refs[i].shape[0] // STORES if refs[i].shape[0] % (16 * STORES) == 0 else refs[i].shape[0]
        for j in range(refs[i].shape[0] // size):
            band = slice(j * size, (j + 1) * size)
            copies.append(pltpu.make_async_copy(refs[i].at[band], refs[count + i].at[band], sems.at[i, j]))
    for copy in copies:
        copy.start()
    for copy in copies:
        copy.wait()


def fast_body(
    n_fs,
    n_tp,
    saved_inputs,
    query_cotangent,
    attn_outputs,
    out_cotangent,
    left_factor,
    right_factor,
    query_master,
    out_master,
    first_moment,
    second_moment,
):
    tokens, model = saved_inputs.shape
    features = query_cotangent.shape[1]
    width, part = left_factor.shape
    depth = first_moment.shape[1]
    rank = part * n_tp
    outer = n_fs // PAIR
    pieces = width // LANES
    slots = 2 * (FACTOR_CUTS + DIRECTION_CUTS + pieces)
    low, wide = jnp.bfloat16, jnp.float32
    vmem = pl.BlockSpec(memory_space=pltpu.VMEM)
    anywhere = pl.BlockSpec(memory_space=pl.ANY)
    dma = pltpu.SemaphoreType.DMA
    results = pl.pallas_call(
        functools.partial(kernel, n_fs, n_tp, EARLY_QUERY, EARLY_OUT),
        out_shape=(
            pltpu.VMEM((width, features), wide),
            pltpu.VMEM((features, width), wide),
            pltpu.VMEM((model, features), low),
            pltpu.VMEM((features, model), low),
            pltpu.VMEM(first_moment.shape, wide),
            pltpu.VMEM(first_moment.shape, wide),
        ),
        in_specs=[anywhere] * 10,
        out_specs=(vmem,) * 6,
        scratch_shapes=[
            pltpu.VMEM((2, part, width), low),
            pltpu.VMEM(first_moment.shape, wide),
            pltpu.VMEM(first_moment.shape, wide),
            pltpu.VMEM((2, rank, model), low),
            pltpu.VMEM((2, rank, width), low),
            pltpu.VMEM((2, rank, features), low),
            pltpu.VMEM((width, features), wide),
            pltpu.VMEM((features, width), wide),
            pltpu.VMEM((max(EARLY_QUERY, 1), LANES, features), low),
            pltpu.VMEM((max(EARLY_OUT, 1), features // pieces, width), low),
            pltpu.VMEM((tokens, model), low),
            pltpu.VMEM((tokens, model), low),
            pltpu.VMEM((tokens, features), low),
            pltpu.VMEM((tokens, features), low),
            pltpu.VMEM((2, rank, tokens), low),
            pltpu.VMEM((2, rank, features), wide),
            pltpu.VMEM((outer, 2, depth, features), low),
            pltpu.VMEM((outer, 2, depth, features), low),
            pltpu.VMEM((outer, 2, depth, features), low),
            pltpu.VMEM((outer, 2, depth, features), low),
            pltpu.VMEM((2, depth, features), low),
            pltpu.VMEM((n_fs + n_tp, 8, 128), wide),
            dma((10,)),
            dma((2, 2, n_tp // PAIR)),
            dma((2, 2, 2, n_tp // PAIR)),
            dma((2, 2, n_tp // PAIR)),
            dma((outer, 2)),
            dma((outer, 2)),
            dma((2,)),
            dma((2, 2)),
            dma((slots,)),
            dma((slots, 5)),
        ],
        compiler_params=pltpu.CompilerParams(
            collective_id=0, has_side_effects=True, vmem_limit_bytes=46 * 2**20
        ),
        cost_estimate=pl.CostEstimate(
            flops=4 * tokens * rank * (model + features), bytes_accessed=200 * 2**20, transcendentals=0
        ),
    )(
        saved_inputs,
        out_cotangent,
        query_cotangent,
        attn_outputs,
        query_master,
        out_master,
        left_factor.T,
        right_factor.T,
        first_moment,
        second_moment,
    )
    return pl.pallas_call(
        store_kernel,
        out_shape=tuple(jax.ShapeDtypeStruct(r.shape, r.dtype) for r in results),
        in_specs=[vmem] * len(results),
        out_specs=(anywhere,) * len(results),
        scratch_shapes=[dma((len(results), STORES))],
        compiler_params=pltpu.CompilerParams(vmem_limit_bytes=2**20),
        cost_estimate=pl.CostEstimate(flops=2**20, bytes_accessed=13 * 2**20, transcendentals=0),
    )(*(pltpu.with_memory_space_constraint(r, pltpu.VMEM) for r in results))


def plain_body(
    saved_inputs,
    query_cotangent,
    attn_outputs,
    out_cotangent,
    left_factor,
    right_factor,
    query_master,
    out_master,
    first_moment,
    second_moment,
):
    left_part = jnp.dot(
        saved_inputs,
        lax.all_gather(left_factor, "fs", axis=0, tiled=True),
        preferred_element_type=jnp.float32,
    )
    right_part = jnp.dot(
        out_cotangent,
        lax.all_gather(right_factor, "fs", axis=0, tiled=True),
        preferred_element_type=jnp.float32,
    )
    left_proj, right_proj, left_rows, right_rows = (
        lax.all_gather(left_part.astype(jnp.bfloat16), "tp", axis=1, tiled=True),
        lax.all_gather(right_part.astype(jnp.bfloat16), "tp", axis=1, tiled=True),
        lax.all_gather(left_factor, "tp", axis=1, tiled=True),
        lax.all_gather(right_factor, "tp", axis=1, tiled=True),
    )
    depth = first_moment.shape[1]
    grad_query = lax.dot_general(left_proj, query_cotangent, TN, preferred_element_type=jnp.float32)
    grad_output = lax.dot_general(right_proj, attn_outputs, TN, preferred_element_type=jnp.float32)
    summed = lax.psum_scatter(
        jnp.stack([grad_query, grad_output], axis=1), "fs", scatter_dimension=0, tiled=True
    )
    grads = jnp.transpose(summed, (1, 0, 2))
    first_new, second_new, own_direction = moment_step(first_moment, second_moment, grads)
    direction_all = lax.all_gather(own_direction.astype(jnp.bfloat16), "fs", axis=1, tiled=True)
    squares = jnp.sum(own_direction * own_direction, axis=(1, 2))
    total = lax.psum(squares, ("fs", "tp"))
    entries = depth * lax.axis_size("fs") * own_direction.shape[2] * lax.axis_size("tp")
    scale = lax.rsqrt(total / entries + 1e-06)
    step_query = scale[0] * jnp.dot(left_rows, direction_all[0], preferred_element_type=jnp.float32)
    step_output = scale[1] * lax.dot_general(
        direction_all[1], right_rows, (((0,), (1,)), ((), ())), preferred_element_type=jnp.float32
    )
    query_new = query_master - 0.01 * step_query
    out_new = out_master - 0.01 * step_output
    query_copy, out_copy = (
        lax.all_gather(query_new.astype(jnp.bfloat16), "fs", axis=0, tiled=True),
        lax.all_gather(out_new.astype(jnp.bfloat16), "fs", axis=1, tiled=True),
    )
    return (query_new, out_new, query_copy, out_copy, first_new, second_new)


def choose_body(n_fs, n_tp, *args):
    left_factor, first_moment = args[4], args[8]
    model, part = args[0].shape[1], left_factor.shape[1]
    aligned = part % (16 * FACTOR_CUTS) == 0 and first_moment.shape[1] % 16 == 0
    aligned = aligned and model // n_fs % 128 == 0 and first_moment.shape[2] % (128 * DIRECTION_CUTS) == 0
    aligned = aligned and first_moment.shape[2] % (model // n_fs) == 0
    if aligned and n_fs == PAIR * LINE and n_tp % PAIR == 0:
        return fast_body(n_fs, n_tp, *args)
    return plain_body(*args)


def solution(mesh):
    return jax.shard_map(
        functools.partial(choose_body, mesh.shape["fs"], mesh.shape["tp"]),
        mesh=mesh,
        in_specs=(
            P("fs", None),
            P("fs", "tp"),
            P("fs", "tp"),
            P("fs", None),
            P("fs", "tp"),
            P("fs", "tp"),
            P("fs", "tp"),
            P("tp", "fs"),
            P(None, "fs", "tp"),
            P(None, "fs", "tp"),
        ),
        out_specs=(
            P("fs", "tp"),
            P("tp", "fs"),
            P(None, "tp"),
            P("tp", None),
            P(None, "fs", "tp"),
            P(None, "fs", "tp"),
        ),
        check_vma=False,
    )
```
